32 devices in a mesh: sp: 2 (over x), dp: 16 (over z, y, core).
Axes of the slice: x: 2, y: 2, z: 4, core: 2. Of those that a mesh axis runs over, the one named last changes fastest.
Arguments:
- hidden_in: bfloat16 [1024, 2048], P('sp'), may hold values from -6 to 6
- content_weight: bfloat16 [2048, 2048], P('sp', 'dp'), may hold values from -0.125 to 0.125
- gating_weight: bfloat16 [2048, 2048], P('sp', 'dp'), may hold values from -2 to 2
- norm_gain: float32 [2048], P('dp'), may hold values from 0.1 to 1.9
- mixing_weight: bfloat16 [16, 128, 128], P('dp'), may hold values from -0.5 to 0.5
- mixing_bias: float32 [16, 128], P('dp'), may hold values from 0.1 to 1.9
- out_grad: bfloat16 [1024, 2048], P('sp', 'dp'), may hold values from -13 to 13
Outputs:
- input_grad: bfloat16 [1024, 2048], P('sp', 'dp')
- content_grad: float32 [2048, 2048], P('sp', 'dp')
- gating_grad: float32 [2048, 2048], P('sp', 'dp')
- mixing_grad: float32 [16, 128, 128], P('dp')
The draws below stay inside these ranges and needn't reach their ends.
All inputs are finite; a program needn't handle non-finite values.
Results may differ from the reference program's by a relative error of at most 0.019.
Values may be sent and summed in bfloat16 or wider, within the bound.
A program may use at most 64 MiB of HBM per device.

```python
import math
import jax
import jax.numpy as jnp
from jax import lax

D = 2048
G = 16
GROUP_DIM = 128
BLOCK = 128
F = 2048
TOKENS = 1024
N_DP = 16


def column_scales(key):
    group_of = (jnp.arange(F) // GROUP_DIM).astype(jnp.float32)
    rising = group_of / (G - 1)
    jitter = jax.random.uniform(key, (F,), jnp.float32)
    exponent = 0.5 * rising + 0.5 * jitter
    return 10.0 ** (exponent - 0.5)


def draw_gating_weight(key, part):
    entries = jax.random.truncated_normal(jax.random.fold_in(key, 11), -4.0, 4.0, (D, F), jnp.float32)
    scales = column_scales(jax.random.fold_in(key, 12))
    return (entries * scales[None, :] * D ** (-0.5)).astype(jnp.bfloat16)


def draw_out_grad(key, part):
    entries = jax.random.truncated_normal(jax.random.fold_in(key, 21), -4.0, 4.0, (TOKENS, F), jnp.float32)
    scales = column_scales(jax.random.fold_in(key, 22))
    return (entries * scales[None, :]).astype(jnp.bfloat16)


def level_of(stream_key, extent, cuts, low, top_value):
    gain = 1.0
    for axis_at, blocks in cuts:
        draws = jax.random.uniform(jax.random.fold_in(jax.random.fold_in(stream_key, 6), axis_at), (blocks,), jnp.float32, low / len(cuts), top_value / len(cuts))
        gain = gain * jnp.repeat(jnp.exp(draws), extent[axis_at] // blocks).reshape((-1,) + (1,) * (len(extent) - 1 - axis_at))
    return gain


def bell_draw(own_key, extent, scale, limit, pieces=(), kind=jnp.bfloat16):
    result = jax.random.normal(own_key, extent, jnp.float32) * scale
    if len(pieces) > 0:
        result = level_of(own_key, extent, pieces, -0.22, 0.18) * result
    return jnp.clip(result, min=-limit, max=limit).astype(kind)


def setup_inputs(seed: int = 0) -> dict:
    seeds = jax.random.split(jax.random.key(seed), 8)
    hidden_in = bell_draw(seeds[0], (TOKENS, D), 1.0, 6.0, ((0, 2),))
    content_weight = bell_draw(seeds[1], (D, F), D ** -0.5, 0.125, ((0, 2), (1, 16)))
    gating_weight = draw_gating_weight(jax.random.fold_in(seeds[7], 71), 0)
    norm_gain = jnp.clip(1.0 + 0.18 * jax.random.normal(seeds[3], (F,), jnp.float32), 0.1, 1.9)
    mixing_weight = bell_draw(seeds[4], (G, BLOCK, BLOCK), BLOCK ** -0.5, 0.5, ((0, 16),))
    mixing_bias = jnp.clip(1.0 + 0.18 * jax.random.normal(seeds[5], (G, BLOCK), jnp.float32), 0.1, 1.9)
    out_grad = draw_out_grad(jax.random.fold_in(seeds[7], 71), 0)
    return dict(hidden_in=hidden_in, content_weight=content_weight, gating_weight=gating_weight, norm_gain=norm_gain, mixing_weight=mixing_weight, mixing_bias=mixing_bias, out_grad=out_grad)


norm_eps = 1e-05

def gelu_slope(values):
    cumulative = 0.5 * (1.0 + lax.erf(values * (1.0 / math.sqrt(2.0))))
    density = jnp.exp(-0.5 * values * values) * (1.0 / math.sqrt(2.0 * math.pi))
    return cumulative + values * density

def stored(values):
    return lax.optimization_barrier(values.astype(jnp.bfloat16))

def causal_table(weights):
    row_ids = lax.broadcasted_iota(jnp.int32, (BLOCK, BLOCK), 0)
    col_ids = lax.broadcasted_iota(jnp.int32, (BLOCK, BLOCK), 1)
    keeper = (col_ids <= row_ids)[None]
    return (jnp.where(keeper, weights, jnp.zeros_like(weights)), keeper)

def reference(hidden_in, content_weight, gating_weight, norm_gain, mixing_weight, mixing_bias, out_grad):
    tokens = hidden_in.shape[0]
    width = content_weight.shape[1]
    groups = width // GROUP_DIM
    blocks = tokens // BLOCK
    grad_scale = 1.0 / math.sqrt(tokens)
    pre_content = stored(jnp.dot(hidden_in, content_weight, preferred_element_type=jnp.float32)).astype(jnp.float32)
    pre_gating = stored(jnp.dot(hidden_in, gating_weight, preferred_element_type=jnp.float32)).astype(jnp.float32)
    content = jax.nn.gelu(pre_content, approximate=False)
    gating = jax.nn.gelu(pre_gating, approximate=False)
    row_mean = lax.optimization_barrier(jnp.mean(gating, axis=1, keepdims=True))
    row_var = lax.optimization_barrier(jnp.mean(gating * gating, axis=1, keepdims=True)) - row_mean * row_mean
    inv_std = lax.rsqrt(row_var + norm_eps)
    centred = (gating - row_mean) * inv_std
    normed = (centred * norm_gain[None, :]).astype(jnp.bfloat16)
    spatial, keeper = causal_table(mixing_weight)
    spatial_wide = spatial.astype(jnp.float32)
    normed_blocks = normed.astype(jnp.float32).reshape(blocks, BLOCK, groups, GROUP_DIM)
    mixed = jnp.einsum('gts,bsgc->btgc', spatial_wide, normed_blocks)
    mixed = mixed + jnp.transpose(mixing_bias)[None, :, :, None]
    mixed = mixed.reshape(tokens, width)
    grad_wide = out_grad.astype(jnp.float32)
    content_pre_grad = (grad_wide * mixed * gelu_slope(pre_content)).astype(jnp.bfloat16)
    mixed_grad = (grad_wide * content).astype(jnp.bfloat16)
    mixed_blocks = mixed_grad.astype(jnp.float32).reshape(blocks, BLOCK, groups, GROUP_DIM)
    mixing_grad = jnp.where(keeper, jnp.einsum('btgc,bsgc->gts', mixed_blocks, normed_blocks), 0.0) * grad_scale
    normed_grad = jnp.einsum('gts,btgc->bsgc', spatial_wide, mixed_blocks).reshape(tokens, width)
    centred_grad = normed_grad * norm_gain[None, :]
    first_moment = lax.optimization_barrier(jnp.mean(centred_grad, axis=1, keepdims=True))
    second_moment = lax.optimization_barrier(jnp.mean(centred_grad * centred, axis=1, keepdims=True))
    gating_back = inv_std * (centred_grad - first_moment - centred * second_moment)
    gating_pre_grad = (gating_back * gelu_slope(pre_gating)).astype(jnp.bfloat16)
    shard_cols = width // N_DP
    dims = (((1,), (1,)), ((), ()))

    def add_shard(running, shard_index):
        col_start = shard_index * shard_cols
        part_content = lax.dynamic_slice_in_dim(content_pre_grad, col_start, shard_cols, 1)
        part_gating = lax.dynamic_slice_in_dim(gating_pre_grad, col_start, shard_cols, 1)
        weight_content = lax.dynamic_slice_in_dim(content_weight, col_start, shard_cols, 1)
        weight_gating = lax.dynamic_slice_in_dim(gating_weight, col_start, shard_cols, 1)
        term = lax.dot_general(part_content, weight_content, dims, preferred_element_type=jnp.float32)
        term = term + lax.dot_general(part_gating, weight_gating, dims, preferred_element_type=jnp.float32)
        return (running + stored(term).astype(jnp.float32), None)
    input_sum, unused = lax.scan(add_shard, jnp.zeros((tokens, D), jnp.float32), jnp.arange(N_DP, dtype=jnp.int32))
    token_dims = (((0,), (0,)), ((), ()))
    content_grad = lax.dot_general(hidden_in, content_pre_grad, token_dims, preferred_element_type=jnp.float32) * grad_scale
    gating_grad = lax.dot_general(hidden_in, gating_pre_grad, token_dims, preferred_element_type=jnp.float32) * grad_scale
    return (input_sum.astype(jnp.bfloat16), content_grad, gating_grad, mixing_grad)
```

```python
import functools
import math

import jax
import jax.numpy as jnp
from jax import lax
from jax.experimental import pallas as pl
from jax.experimental.pallas import tpu as pltpu
from jax.sharding import PartitionSpec as P

GROUP_DIM = 128
BLOCK = 128


norm_eps = 1e-05


def gelu_slope(values):
    cumulative = 0.5 * (1.0 + lax.erf(values * (1.0 / math.sqrt(2.0))))
    density = jnp.exp(-0.5 * values * values) * (1.0 / math.sqrt(2.0 * math.pi))
    return cumulative + values * density


def causal_table(weights):
    row_ids = lax.broadcasted_iota(jnp.int32, (BLOCK, BLOCK), 0)
    col_ids = lax.broadcasted_iota(jnp.int32, (BLOCK, BLOCK), 1)
    keeper = (col_ids <= row_ids)[None]
    return (jnp.where(keeper, weights, jnp.zeros_like(weights)), keeper)


def hidden_term(hidden_in, grads):
    return lax.dot_general(
        hidden_in, grads, (((0,), (0,)), ((), ())), preferred_element_type=jnp.float32
    )


def local(
    hidden_in, content_weight, gating_weight, norm_gain, mixing_weight, mixing_bias, out_grad
):
    tok_rows = hidden_in.shape[0]
    local_width = content_weight.shape[1]
    groups_here = local_width // GROUP_DIM
    blocks = tok_rows // BLOCK
    full_width = local_width * lax.axis_size("dp")
    grad_scale = 1.0 / math.sqrt(tok_rows * lax.axis_size("sp"))
    whole_content, whole_gating = (
        lax.all_gather(content_weight, "sp", axis=0, tiled=True),
        lax.all_gather(gating_weight, "sp", axis=0, tiled=True),
    )
    joined_weight = jnp.concatenate([whole_content, whole_gating], axis=1)
    pre_both = jnp.dot(hidden_in, joined_weight, preferred_element_type=jnp.float32).astype(
        jnp.bfloat16
    )
    pre_content = pre_both[:, :local_width].astype(jnp.float32)
    pre_gating = pre_both[:, local_width:].astype(jnp.float32)
    content = jax.nn.gelu(pre_content, approximate=False)
    gating = jax.nn.gelu(pre_gating, approximate=False)
    spatial, keeper = causal_table(mixing_weight)
    grad_wide = out_grad.astype(jnp.float32)
    mixed_grad = (grad_wide * content).astype(jnp.bfloat16)
    mixed_blocks = mixed_grad.reshape(blocks, BLOCK, groups_here, GROUP_DIM)
    normed_grad = jnp.einsum(
        "gts,btgc->bsgc", spatial, mixed_blocks, preferred_element_type=jnp.float32
    )
    centred_grad = normed_grad.reshape(tok_rows, local_width) * norm_gain[None, :]
    row_sum, row_square, grad_sum, grad_raw = lax.psum(
        (
            jnp.sum(gating, axis=1),
            jnp.sum(gating * gating, axis=1),
            jnp.sum(centred_grad, axis=1),
            jnp.sum(centred_grad * gating, axis=1),
        ),
        "dp",
    )
    row_mean = (row_sum / full_width)[:, None]
    row_var = (row_square / full_width)[:, None] - row_mean * row_mean
    inv_std = lax.rsqrt(row_var + norm_eps)
    centred = (gating - row_mean) * inv_std
    first_moment = (grad_sum / full_width)[:, None]
    second_moment = inv_std * ((grad_raw / full_width)[:, None] - row_mean * first_moment)
    normed = (centred * norm_gain[None, :]).astype(jnp.bfloat16)
    normed_blocks = normed.reshape(blocks, BLOCK, groups_here, GROUP_DIM)
    mixed = jnp.einsum("gts,bsgc->btgc", spatial, normed_blocks, preferred_element_type=jnp.float32)
    mixed = (mixed + jnp.transpose(mixing_bias)[None, :, :, None]).reshape(tok_rows, local_width)
    content_pre_grad = (grad_wide * mixed * gelu_slope(pre_content)).astype(jnp.bfloat16)
    local_mixing = jnp.einsum(
        "btgc,bsgc->gts", mixed_blocks, normed_blocks, preferred_element_type=jnp.float32
    )
    local_mixing = jnp.where(keeper, local_mixing, 0.0)
    mixing_grad = lax.psum(local_mixing.astype(jnp.bfloat16), "sp").astype(jnp.float32) * grad_scale
    gating_back = inv_std * (centred_grad - first_moment - centred * second_moment)
    gating_pre_grad = (gating_back * gelu_slope(pre_gating)).astype(jnp.bfloat16)
    joined_grad = jnp.concatenate([content_pre_grad, gating_pre_grad], axis=1)
    partial_input = lax.dot_general(
        joined_grad, joined_weight, (((1,), (1,)), ((), ())), preferred_element_type=jnp.float32
    )
    input_grad = lax.psum_scatter(
        partial_input.astype(jnp.bfloat16), "dp", scatter_dimension=1, tiled=True
    )
    both_grads = (
        lax.psum_scatter(
            hidden_term(hidden_in, joined_grad).astype(jnp.bfloat16),
            "sp",
            scatter_dimension=0,
            tiled=True,
        ).astype(jnp.float32)
        * grad_scale
    )
    content_grad = both_grads[:, :local_width]
    gating_grad = both_grads[:, local_width:]
    return (input_grad, content_grad, gating_grad, mixing_grad)


def phi_and_slope(values):
    cumulative = 0.5 * (1.0 + lax.erf(values * (1.0 / math.sqrt(2.0))))
    density = jnp.exp(-0.5 * values * values) * (1.0 / math.sqrt(2.0 * math.pi))
    return cumulative, cumulative + values * density


def dot(a, b, ca, cb):
    return lax.dot_general(
        a, b, (((ca,), (cb,)), ((), ())), preferred_element_type=jnp.float32
    )


def fused_kernel(
    n_dp, full_width, grad_scale,
    h_in, wc_in, wg_in, gain_in, mix_in, bias_in, og_in,
    x_out, c_out, g_out, m_out,
    gain_ref, mix_ref, bias_ref, hid, hid_t, wts, og, cg, cg_t, cs, gat, slope_g, mg, joined,
    stat_a, stat_quad, stat_b, stat_z,
    part, r_core, q_send, r_y, z_send, r_z, acc,
    gs, gr, go, ms, mr,
    load_sem, w_send, w_recv, sq_send, sq_recv, sz_send, sz_recv,
    core_send, core_recv, y_send, y_recv, zz_send, zz_recv,
    gx_send, gx_recv, mx_send, mx_recv,
):
    toks = hid.shape[0]
    chunks = toks // BLOCK
    shard = wc_in.shape[0]
    nz = n_dp // 4
    half = toks // 2
    tiles = gs.shape[0]
    tile = gs.shape[1]
    bf16 = jnp.bfloat16
    f32 = jnp.float32

    i = lax.axis_index("sp")
    j = lax.axis_index("dp")
    x_peer = 1 - i
    c = lax.rem(j, 2)
    y = lax.rem(j // 2, 2)
    z = j // 4
    j_core = j + 1 - 2 * c
    j_y = j + 2 - 4 * y
    j_diag = j_core + 2 - 4 * y

    mid = lax.rem((z + 1) // 2, 2)
    z_xor = (z, z + 1 - 2 * lax.rem(z, 2), z + 2 - 4 * (z // 2), 3 - z)

    def z_dev(q):
        return z_xor[q] * 4 + y * 2 + c

    def dev(a, b):
        return {"sp": a, "dp": b}

    def remote(src, dst, ssem, rsem, target):
        return pltpu.make_async_remote_copy(
            src_ref=src, dst_ref=dst, send_sem=ssem, recv_sem=rsem,
            device_id=target, device_id_type=pl.DeviceIdType.MESH,
        )

    mine = pl.multiple_of(i * shard, shard)
    theirs = pl.multiple_of(x_peer * shard, shard)
    loads = [
        pltpu.make_async_copy(wc_in, wts.at[pl.ds(mine, shard), pl.ds(0, BLOCK)], load_sem.at[0]),
        pltpu.make_async_copy(h_in, hid, load_sem.at[1]),
        pltpu.make_async_copy(wg_in, wts.at[pl.ds(mine, shard), pl.ds(BLOCK, BLOCK)], load_sem.at[2]),
        pltpu.make_async_copy(og_in, og, load_sem.at[3]),
        pltpu.make_async_copy(gain_in, gain_ref, load_sem.at[4]),
        pltpu.make_async_copy(mix_in, mix_ref, load_sem.at[5]),
        pltpu.make_async_copy(bias_in, bias_ref, load_sem.at[6]),
    ]
    for load in loads:
        load.start()

    barrier = pltpu.get_barrier_semaphore()
    peers = [dev(x_peer, j), dev(i, j_core), dev(i, j_y), dev(i, j_diag)]
    peers += [dev(i, z_dev(q)) for q in range(1, nz)]
    for peer in peers:
        pl.semaphore_signal(barrier, inc=1, device_id=peer, device_id_type=pl.DeviceIdType.MESH)
    pl.semaphore_wait(barrier, len(peers))

    pieces = w_send.shape[0] // 2
    piece = shard // pieces
    w_copies = []
    for which, src in ((0, wc_in), (1, wg_in)):
        for p in range(pieces):
            copy = remote(
                src.at[pl.ds(p * piece, piece), :],
                wts.at[pl.ds(pl.multiple_of(mine + p * piece, piece), piece), pl.ds(which * BLOCK, BLOCK)],
                w_send.at[which * pieces + p], w_recv.at[which * pieces + p],
                dev(x_peer, j),
            )
            copy.start()
            w_copies.append(copy)

    keep = lax.broadcasted_iota(jnp.int32, (BLOCK, BLOCK), 1) <= lax.broadcasted_iota(
        jnp.int32, (BLOCK, BLOCK), 0
    )
    for load in loads:
        load.wait()
    spatial = jnp.where(keep, mix_ref[0].astype(f32), 0.0).astype(bf16)
    gain = gain_ref[...]
    bias = jnp.broadcast_to(bias_ref[...], (BLOCK, BLOCK)).T
    own = dot(hid[:, pl.ds(mine, shard)], wts[pl.ds(mine, shard), :], 1, 0)
    joined_pre = own
    acc_c = go.at[pl.ds(0, toks), pl.ds(0, BLOCK)]
    acc_g = go.at[pl.ds(0, toks), pl.ds(BLOCK, BLOCK)]
    go[pl.ds(0, toks), :] = joined_pre
    for b in range(hid.shape[1] // BLOCK):
        hid_t[pl.ds(b * BLOCK, BLOCK), :] = hid[:, pl.ds(b * BLOCK, BLOCK)].T

    def finish(which, target):
        for p in range(pieces):
            w_copies[which * pieces + p].wait_recv()
            at = pl.multiple_of(theirs + p * piece, piece)
            target[...] += dot(
                hid[:, pl.ds(at, piece)], wts[pl.ds(at, piece), pl.ds(which * BLOCK, BLOCK)], 1, 0
            )

    finish(0, acc_c)
    for k in range(chunks):
        rows = pl.ds(k * BLOCK, BLOCK)
        pre = go[rows, 0:BLOCK].astype(bf16).astype(f32)
        wide = og[rows, :].astype(f32)
        cumulative, slope = phi_and_slope(pre)
        cs[rows, :] = wide * slope
        mixed_grad = (wide * (pre * cumulative)).astype(bf16)
        mg[rows, :] = mixed_grad
        centred_grad = dot(spatial, mixed_grad, 0, 0) * gain
        cg[rows, :] = centred_grad
        cg_t[rows, :] = centred_grad.T

    finish(1, acc_g)
    for k in range(chunks):
        rows = pl.ds(k * BLOCK, BLOCK)
        pre = go[rows, BLOCK:2 * BLOCK].astype(bf16).astype(f32)
        cumulative, slope = phi_and_slope(pre)
        gating = pre * cumulative
        gat[rows, :] = gating
        slope_g[rows, :] = slope
        turned = gating.T
        grad_turned = cg_t[rows, :]
        base = 4 * (k * BLOCK // half)
        cols = pl.ds(k * BLOCK % half, BLOCK)
        for row, table in enumerate((turned, turned * turned, grad_turned, grad_turned * turned)):
            stat_a[base + row:base + row + 1, cols] = jnp.sum(table, axis=0, keepdims=True)

    stat_copies = []
    for s, target in enumerate((j_core, j_y, j_diag)):
        copy = remote(stat_a, stat_quad.at[s], sq_send.at[s], sq_recv.at[s], dev(i, target))
        copy.start()
        stat_copies.append(copy)
    for copy in stat_copies:
        copy.wait()
    stat_b[...] = (stat_a[...] + stat_quad[0]) + (stat_quad[1] + stat_quad[2])
    stat_copies = []
    for q in range(1, nz):
        copy = remote(
            stat_b, stat_z.at[q - 1], sz_send.at[q - 1], sz_recv.at[q - 1], dev(i, z_dev(q))
        )
        copy.start()
        stat_copies.append(copy)
    for copy in stat_copies:
        copy.wait()
    total = stat_b[...]
    for q in range(1, nz):
        total = total + stat_z[q - 1]
    total = total * (1.0 / full_width)

    mixing = jnp.zeros((BLOCK, BLOCK), f32)
    for k in range(chunks):
        rows = pl.ds(k * BLOCK, BLOCK)
        base = 4 * (k * BLOCK // half)
        col = k * BLOCK % half
        part_of = total[base:base + 4, col:col + BLOCK]
        mean = part_of[0:1]
        inv = lax.rsqrt(part_of[1:2] - mean * mean + norm_eps)
        first = part_of[2:3]
        second = inv * (part_of[3:4] - mean * first)

        def spread(row):
            return jnp.broadcast_to(row, (BLOCK, BLOCK)).T

        inv_w = spread(inv)
        centred = (gat[rows, :] - spread(mean)) * inv_w
        normed = (centred * gain).astype(bf16)
        mixed = dot(spatial, normed, 1, 0) + bias
        joined[rows, 0:BLOCK] = (cs[rows, :] * mixed).astype(bf16)
        back = inv_w * (cg[rows, :] - spread(first) - centred * spread(second))
        joined[rows, BLOCK:2 * BLOCK] = (back * slope_g[rows, :]).astype(bf16)
        mixing = mixing + dot(mg[rows, :], normed, 1, 1)
    mixing = jnp.where(keep, mixing, 0.0)

    waits = []

    order = [(slot, h) for slot in range(nz) for h in range(2)]
    pieces_in = len(order)

    def input_part(n):
        slot, h = order[n]
        grads = joined[pl.ds(h * half, half), :]
        at = pl.multiple_of(z_xor[3 - slot] * (4 * BLOCK), 4 * BLOCK)
        res = dot(grads, wts[pl.ds(at, 4 * BLOCK), :], 1, 1).astype(bf16)
        for yy in range(2):
            for cc in range(2):
                at = (yy * 2 + cc) * BLOCK
                part[n, cc, yy] = res[:, at:at + BLOCK]
        copy = remote(part.at[n, 1 - c], r_core.at[n], core_send.at[n], core_recv.at[n], dev(i, j_core))
        copy.start()
        waits.append(copy)
        core_copies[n] = copy

    def weight_part(t):
        at = pl.multiple_of(theirs + t * tile, tile)
        gs[t] = dot(hid_t[pl.ds(at, tile), :], joined[...], 1, 0).astype(bf16)
        copy = remote(gs.at[t], gr.at[t], gx_send.at[t], gx_recv.at[t], dev(x_peer, j))
        copy.start()
        waits.append(copy)
        return copy

    core_copies, y_copies, z_copies, g_copies = {}, {}, {}, {}

    def second_stage(n):
        core_copies[n].wait_recv()
        q_send[n] = (part[n, c, 1 - y].astype(f32) + r_core[n, 1 - y].astype(f32)).astype(bf16)
        copy = remote(q_send.at[n], r_y.at[n], y_send.at[n], y_recv.at[n], dev(i, j_y))
        copy.start()
        waits.append(copy)
        y_copies[n] = copy

    def direct(h):
        return remote(z_send.at[0, h], r_z.at[0, h], zz_send.at[0, h], zz_recv.at[0, h], dev(i, z_dev(3)))

    def relay(h):
        return remote(z_send.at[0, h], r_z.at[3, h], zz_send.at[0, h], zz_recv.at[3, h], dev(i, z_dev(1)))

    def third_stage(n):
        slot, h = order[n]
        y_copies[n].wait_recv()
        res = (part[n, c, y].astype(f32) + r_core[n, y].astype(f32)) + r_y[n].astype(f32)
        if slot == nz - 1:
            acc[h] = res
            return
        if slot == 0:
            z_send[0, h] = res.astype(bf16)

            @pl.when(mid == 1)
            def _():
                direct(h).start()

            @pl.when(mid == 0)
            def _():
                relay(h).start()

            waits.append(direct(h))
            return
        if slot == 1:

            @pl.when(mid == 1)
            def _():
                relay(h).wait_recv()
                z_send[1, h] = (res + r_z[3, h].astype(f32)).astype(bf16)

            @pl.when(mid == 0)
            def _():
                z_send[1, h] = res.astype(bf16)
        else:
            z_send[slot, h] = res.astype(bf16)
        copy = remote(
            z_send.at[slot, h], r_z.at[slot, h], zz_send.at[slot, h], zz_recv.at[slot, h], dev(i, z_dev(3 - slot))
        )
        copy.start()
        waits.append(copy)
        z_copies[slot, h] = copy

    def last_stage(h):
        @pl.when(mid == 1)
        def _():
            direct(h).wait_recv()
            acc[h] = acc[h] + r_z[0, h].astype(f32)

        res = acc[h]
        for slot in range(1, nz - 1):
            z_copies[slot, h].wait_recv()
            res = res + r_z[slot, h].astype(f32)
        x_out[pl.ds(h * half, half), :] = res.astype(bf16)

    for step in range(pieces_in + 2):
        if step < pieces_in:
            input_part(step)
        if step < tiles:
            g_copies[step] = weight_part(step)
        if step >= 2:
            second_stage(step - 2)
    ms[...] = mixing.astype(bf16)
    m_copy = remote(ms, mr, mx_send, mx_recv, dev(x_peer, j))
    m_copy.start()
    waits.append(m_copy)
    for t in range(tiles):
        at = pl.multiple_of(mine + t * tile, tile)
        go[pl.ds(t * tile, tile), :] = dot(hid_t[pl.ds(at, tile), :], joined[...], 1, 0)
    for n in range(pieces_in):
        third_stage(n)
    for t in range(tiles):
        g_copies[t].wait_recv()
        rows = pl.ds(t * tile, tile)
        done = (go[rows, :] + gr[t].astype(f32)) * grad_scale
        c_out[rows, :] = done[:, 0:BLOCK]
        g_out[rows, :] = done[:, BLOCK:2 * BLOCK]
    m_copy.wait_recv()
    m_out[0] = (mixing + mr[...].astype(f32)) * grad_scale
    for h in range(2):
        last_stage(h)
    for copy in w_copies + waits:
        copy.wait_send()


def store_kernel(*refs):
    count = len(refs) // 2
    src, dst, sem = refs[:count], refs[count:2 * count], refs[-1]
    stores = [pltpu.make_async_copy(src[k], dst[k], sem.at[k]) for k in range(count)]
    for store in stores:
        store.start()
    for store in stores:
        store.wait()


def fused(n_dp, hidden_in, content_weight, gating_weight, norm_gain, mixing_weight, mixing_bias, out_grad):
    toks, depth = hidden_in.shape
    shard, width = content_weight.shape
    half = toks // 2
    nz = n_dp // 4
    tile = 256
    tiles = shard // tile
    pieces = 2
    grad_scale = 1.0 / math.sqrt(2 * toks)
    bf16, f32 = jnp.bfloat16, jnp.float32
    in_hbm = pl.BlockSpec(memory_space=pltpu.HBM)
    dma = pltpu.SemaphoreType.DMA
    V = pltpu.VMEM
    scratch = [
        V((1, width), f32), V((1, BLOCK, BLOCK), bf16), V((1, BLOCK), f32),
        V((toks, depth), bf16), V((depth, toks), bf16), V((depth, 2 * width), bf16), V((toks, width), bf16),
        V((toks, width), f32), V((toks, width), f32), V((toks, width), f32), V((toks, width), f32),
        V((toks, width), f32), V((toks, width), bf16), V((toks, 2 * width), bf16),
        V((8, toks // 2), f32), V((3, 8, toks // 2), f32), V((8, toks // 2), f32), V((nz - 1, 8, toks // 2), f32),
        V((2 * nz, 2, 2, half, width), bf16), V((2 * nz, 2, half, width), bf16),
        V((2 * nz, half, width), bf16), V((2 * nz, half, width), bf16),
        V((nz - 1, 2, half, width), bf16), V((nz, 2, half, width), bf16), V((2, half, width), f32),
        V((tiles, tile, 2 * width), bf16), V((tiles, tile, 2 * width), bf16), V((shard, 2 * width), f32),
        V((BLOCK, BLOCK), bf16), V((BLOCK, BLOCK), bf16),
        dma((7,)), dma((2 * pieces,)), dma((2 * pieces,)), dma((3,)), dma((3,)), dma((nz - 1,)), dma((nz - 1,)),
        dma((2 * nz,)), dma((2 * nz,)), dma((2 * nz,)), dma((2 * nz,)), dma((nz - 1, 2)), dma((nz, 2)),
        dma((tiles,)), dma((tiles,)), dma, dma,
    ]
    results = pl.pallas_call(
        functools.partial(fused_kernel, n_dp, width * n_dp, grad_scale),
        out_shape=(
            V((toks, width), bf16),
            V((shard, width), f32),
            V((shard, width), f32),
            V(mixing_weight.shape, f32),
        ),
        in_specs=[in_hbm] * 7,
        out_specs=(pl.BlockSpec(memory_space=pltpu.VMEM),) * 4,
        scratch_shapes=scratch,
        compiler_params=pltpu.CompilerParams(
            collective_id=0, has_side_effects=True, vmem_limit_bytes=60*1024*1024
        ),
    )(hidden_in, content_weight, gating_weight, norm_gain[None, :], mixing_weight, mixing_bias, out_grad)
    return pl.pallas_call(
        store_kernel,
        out_shape=tuple(jax.ShapeDtypeStruct(r.shape, r.dtype) for r in results),
        in_specs=[pl.BlockSpec(memory_space=pltpu.VMEM)] * 4,
        out_specs=(in_hbm,) * 4,
        scratch_shapes=[dma((4,))],
    )(*[pltpu.with_memory_space_constraint(r, pltpu.VMEM) for r in results])


def fits(n_sp, n_dp, toks, shard, width):
    paired = n_sp == 2 and n_dp == 16
    return paired and width == GROUP_DIM and shard % 512 == 0 and toks % (2 * BLOCK) == 0 and toks <= shard


def solve(*args):
    n_sp, n_dp = lax.axis_size("sp"), lax.axis_size("dp")
    shard, width = args[1].shape
    if fits(n_sp, n_dp, args[0].shape[0], shard, width) and args[0].shape[1] == n_dp * width:
        return fused(n_dp, *args)
    return local(*args)


def solution(mesh):
    in_specs = (
        P("sp", None),
        P("sp", "dp"),
        P("sp", "dp"),
        P("dp"),
        P("dp", None, None),
        P("dp", None),
        P("sp", "dp"),
    )
    out_specs = (P("sp", "dp"), P("sp", "dp"), P("sp", "dp"), P("dp", None, None))
    return jax.shard_map(solve, mesh=mesh, in_specs=in_specs, out_specs=out_specs, check_vma=False)
```

```python
import functools
import math

import jax
import jax.numpy as jnp
from jax import lax
from jax.experimental import pallas as pl
from jax.experimental.pallas import tpu as pltpu
from jax.sharding import PartitionSpec as P

GROUP_DIM = 128
BLOCK = 128


norm_eps = 1e-05


def gelu_slope(values):
    cumulative = 0.5 * (1.0 + lax.erf(values * (1.0 / math.sqrt(2.0))))
    density = jnp.exp(-0.5 * values * values) * (1.0 / math.sqrt(2.0 * math.pi))
    return cumulative + values * density


def causal_table(weights):
    row_ids = lax.broadcasted_iota(jnp.int32, (BLOCK, BLOCK), 0)
    col_ids = lax.broadcasted_iota(jnp.int32, (BLOCK, BLOCK), 1)
    keeper = (col_ids <= row_ids)[None]
    return (jnp.where(keeper, weights, jnp.zeros_like(weights)), keeper)


def hidden_term(hidden_in, grads):
    return lax.dot_general(
        hidden_in, grads, (((0,), (0,)), ((), ())), preferred_element_type=jnp.float32
    )


def local(
    hidden_in, content_weight, gating_weight, norm_gain, mixing_weight, mixing_bias, out_grad
):
    tok_rows = hidden_in.shape[0]
    local_width = content_weight.shape[1]
    groups_here = local_width // GROUP_DIM
    blocks = tok_rows // BLOCK
    full_width = local_width * lax.axis_size("dp")
    grad_scale = 1.0 / math.sqrt(tok_rows * lax.axis_size("sp"))
    whole_content, whole_gating = (
        lax.all_gather(content_weight, "sp", axis=0, tiled=True),
        lax.all_gather(gating_weight, "sp", axis=0, tiled=True),
    )
    joined_weight = jnp.concatenate([whole_content, whole_gating], axis=1)
    pre_both = jnp.dot(hidden_in, joined_weight, preferred_element_type=jnp.float32).astype(
        jnp.bfloat16
    )
    pre_content = pre_both[:, :local_width].astype(jnp.float32)
    pre_gating = pre_both[:, local_width:].astype(jnp.float32)
    content = jax.nn.gelu(pre_content, approximate=False)
    gating = jax.nn.gelu(pre_gating, approximate=False)
    spatial, keeper = causal_table(mixing_weight)
    grad_wide = out_grad.astype(jnp.float32)
    mixed_grad = (grad_wide * content).astype(jnp.bfloat16)
    mixed_blocks = mixed_grad.reshape(blocks, BLOCK, groups_here, GROUP_DIM)
    normed_grad = jnp.einsum(
        "gts,btgc->bsgc", spatial, mixed_blocks, preferred_element_type=jnp.float32
    )
    centred_grad = normed_grad.reshape(tok_rows, local_width) * norm_gain[None, :]
    row_sum, row_square, grad_sum, grad_raw = lax.psum(
        (
            jnp.sum(gating, axis=1),
            jnp.sum(gating * gating, axis=1),
            jnp.sum(centred_grad, axis=1),
            jnp.sum(centred_grad * gating, axis=1),
        ),
        "dp",
    )
    row_mean = (row_sum / full_width)[:, None]
    row_var = (row_square / full_width)[:, None] - row_mean * row_mean
    inv_std = lax.rsqrt(row_var + norm_eps)
    centred = (gating - row_mean) * inv_std
    first_moment = (grad_sum / full_width)[:, None]
    second_moment = inv_std * ((grad_raw / full_width)[:, None] - row_mean * first_moment)
    normed = (centred * norm_gain[None, :]).astype(jnp.bfloat16)
    normed_blocks = normed.reshape(blocks, BLOCK, groups_here, GROUP_DIM)
    mixed = jnp.einsum("gts,bsgc->btgc", spatial, normed_blocks, preferred_element_type=jnp.float32)
    mixed = (mixed + jnp.transpose(mixing_bias)[None, :, :, None]).reshape(tok_rows, local_width)
    content_pre_grad = (grad_wide * mixed * gelu_slope(pre_content)).astype(jnp.bfloat16)
    local_mixing = jnp.einsum(
        "btgc,bsgc->gts", mixed_blocks, normed_blocks, preferred_element_type=jnp.float32
    )
    local_mixing = jnp.where(keeper, local_mixing, 0.0)
    mixing_grad = lax.psum(local_mixing.astype(jnp.bfloat16), "sp").astype(jnp.float32) * grad_scale
    gating_back = inv_std * (centred_grad - first_moment - centred * second_moment)
    gating_pre_grad = (gating_back * gelu_slope(pre_gating)).astype(jnp.bfloat16)
    joined_grad = jnp.concatenate([content_pre_grad, gating_pre_grad], axis=1)
    partial_input = lax.dot_general(
        joined_grad, joined_weight, (((1,), (1,)), ((), ())), preferred_element_type=jnp.float32
    )
    input_grad = lax.psum_scatter(
        partial_input.astype(jnp.bfloat16), "dp", scatter_dimension=1, tiled=True
    )
    both_grads = (
        lax.psum_scatter(
            hidden_term(hidden_in, joined_grad).astype(jnp.bfloat16),
            "sp",
            scatter_dimension=0,
            tiled=True,
        ).astype(jnp.float32)
        * grad_scale
    )
    content_grad = both_grads[:, :local_width]
    gating_grad = both_grads[:, local_width:]
    return (input_grad, content_grad, gating_grad, mixing_grad)


def phi_and_slope(values):
    cumulative = 0.5 * (1.0 + lax.erf(values * (1.0 / math.sqrt(2.0))))
    density = jnp.exp(-0.5 * values * values) * (1.0 / math.sqrt(2.0 * math.pi))
    return cumulative, cumulative + values * density


def dot(a, b, ca, cb):
    return lax.dot_general(
        a, b, (((ca,), (cb,)), ((), ())), preferred_element_type=jnp.float32
    )


def fused_kernel(
    n_dp, full_width, grad_scale,
    h_in, wc_in, wg_in, gain_in, mix_in, bias_in, og_in,
    x_out, c_out, g_out, m_out,
    gain_ref, mix_ref, bias_ref, hid, hid_t, wts, og, cg, cg_t, cs, gat, slope_g, mg, joined,
    stat_a, stat_r,
    part, r_core, q_send, r_y, z_send, r_z, acc,
    gs, gr, go, ms, mr,
    load_sem, w_send, w_recv, st_send, st_recv, hello,
    core_send, core_recv, y_send, y_recv, zz_send, zz_recv,
    gx_send, gx_recv, mx_send, mx_recv,
):
    toks = hid.shape[0]
    chunks = toks // BLOCK
    shard = wc_in.shape[0]
    nz = n_dp // 4
    half = toks // 2
    tiles = gs.shape[0]
    tile = gs.shape[1]
    bf16 = jnp.bfloat16
    f32 = jnp.float32

    i = lax.axis_index("sp")
    j = lax.axis_index("dp")
    x_peer = 1 - i
    c = lax.rem(j, 2)
    y = lax.rem(j // 2, 2)
    z = j // 4
    j_core = j + 1 - 2 * c
    j_y = j + 2 - 4 * y
    j_diag = j_core + 2 - 4 * y

    mid = lax.rem((z + 1) // 2, 2)
    z_xor = (z, z + 1 - 2 * lax.rem(z, 2), z + 2 - 4 * (z // 2), 3 - z)

    def z_dev(q):
        return z_xor[q] * 4 + y * 2 + c

    def dev(a, b):
        return {"sp": a, "dp": b}

    def remote(src, dst, ssem, rsem, target):
        return pltpu.make_async_remote_copy(
            src_ref=src, dst_ref=dst, send_sem=ssem, recv_sem=rsem,
            device_id=target, device_id_type=pl.DeviceIdType.MESH,
        )

    mine = pl.multiple_of(i * shard, shard)
    theirs = pl.multiple_of(x_peer * shard, shard)
    loads = [
        pltpu.make_async_copy(wc_in, wts.at[pl.ds(mine, shard), pl.ds(0, BLOCK)], load_sem.at[0]),
        pltpu.make_async_copy(h_in, hid, load_sem.at[1]),
        pltpu.make_async_copy(wg_in, wts.at[pl.ds(mine, shard), pl.ds(BLOCK, BLOCK)], load_sem.at[2]),
        pltpu.make_async_copy(og_in, og, load_sem.at[3]),
        pltpu.make_async_copy(gain_in, gain_ref, load_sem.at[4]),
        pltpu.make_async_copy(mix_in, mix_ref, load_sem.at[5]),
        pltpu.make_async_copy(bias_in, bias_ref, load_sem.at[6]),
    ]
    for load in loads:
        load.start()

    def tell(sem, target):
        pl.semaphore_signal(sem, inc=1, device_id=target, device_id_type=pl.DeviceIdType.MESH)

    barrier = pltpu.get_barrier_semaphore()

    @pl.when(i == 0)
    def _():
        tell(barrier, dev(x_peer, j))

    @pl.when(i == 1)
    def _():
        pl.semaphore_wait(barrier, 1)
        tell(hello, dev(x_peer, j))

    @pl.when(i == 0)
    def _():
        pl.semaphore_wait(hello, 1)

    pieces = w_send.shape[0] // 2
    piece = shard // pieces
    w_copies = []
    for which, src in ((0, wc_in), (1, wg_in)):
        for p in range(pieces):
            copy = remote(
                src.at[pl.ds(p * piece, piece), :],
                wts.at[pl.ds(pl.multiple_of(mine + p * piece, piece), piece), pl.ds(which * BLOCK, BLOCK)],
                w_send.at[which * pieces + p], w_recv.at[which * pieces + p],
                dev(x_peer, j),
            )
            copy.start()
            w_copies.append(copy)

    others = [dev(i, lax.rem(j + k, n_dp)) for k in range(1, n_dp)]

    @pl.when(i == 0)
    def _():
        for target in others:
            tell(barrier, target)
        pl.semaphore_wait(barrier, len(others))
        tell(hello, dev(x_peer, j))

    @pl.when(i == 1)
    def _():
        pl.semaphore_wait(hello, 1)

    keep = lax.broadcasted_iota(jnp.int32, (BLOCK, BLOCK), 1) <= lax.broadcasted_iota(
        jnp.int32, (BLOCK, BLOCK), 0
    )
    for load in loads:
        load.wait()
    spatial = jnp.where(keep, mix_ref[0].astype(f32), 0.0).astype(bf16)
    gain = gain_ref[...]
    bias = jnp.broadcast_to(bias_ref[...], (BLOCK, BLOCK)).T
    own = dot(hid[:, pl.ds(mine, shard)], wts[pl.ds(mine, shard), :], 1, 0)
    joined_pre = own
    acc_c = go.at[pl.ds(0, toks), pl.ds(0, BLOCK)]
    acc_g = go.at[pl.ds(0, toks), pl.ds(BLOCK, BLOCK)]
    go[pl.ds(0, toks), :] = joined_pre
    for b in range(hid.shape[1] // BLOCK):
        hid_t[pl.ds(b * BLOCK, BLOCK), :] = hid[:, pl.ds(b * BLOCK, BLOCK)].T

    def finish(which, target):
        for p in range(pieces):
            w_copies[which * pieces + p].wait_recv()
            at = pl.multiple_of(theirs + p * piece, piece)
            target[...] += dot(
                hid[:, pl.ds(at, piece)], wts[pl.ds(at, piece), pl.ds(which * BLOCK, BLOCK)], 1, 0
            )

    finish(0, acc_c)
    for k in range(chunks):
        rows = pl.ds(k * BLOCK, BLOCK)
        pre = go[rows, 0:BLOCK].astype(bf16).astype(f32)
        wide = og[rows, :].astype(f32)
        cumulative, slope = phi_and_slope(pre)
        cs[rows, :] = wide * slope
        mixed_grad = (wide * (pre * cumulative)).astype(bf16)
        mg[rows, :] = mixed_grad
        centred_grad = dot(spatial, mixed_grad, 0, 0) * gain
        cg[rows, :] = centred_grad
        cg_t[rows, :] = centred_grad.T

    finish(1, acc_g)
    for k in range(chunks):
        rows = pl.ds(k * BLOCK, BLOCK)
        pre = go[rows, BLOCK:2 * BLOCK].astype(bf16).astype(f32)
        cumulative, slope = phi_and_slope(pre)
        gating = pre * cumulative
        gat[rows, :] = gating
        slope_g[rows, :] = slope
        turned = gating.T
        grad_turned = cg_t[rows, :]
        base = 4 * (k * BLOCK // half)
        cols = pl.ds(k * BLOCK % half, BLOCK)
        for row, table in enumerate((turned, turned * turned, grad_turned, grad_turned * turned)):
            stat_a[base + row:base + row + 1, cols] = jnp.sum(table, axis=0, keepdims=True)

    stat_copies = []
    for k, target in enumerate(others):
        copy = remote(stat_a, stat_r.at[k], st_send.at[k], st_recv.at[k], target)
        copy.start()
        stat_copies.append(copy)
    total = stat_a[...]
    for k, copy in enumerate(stat_copies):
        copy.wait_recv()
        total = total + stat_r[k]
    total = total * (1.0 / full_width)

    mixing = jnp.zeros((BLOCK, BLOCK), f32)
    for k in range(chunks):
        rows = pl.ds(k * BLOCK, BLOCK)
        base = 4 * (k * BLOCK // half)
        col = k * BLOCK % half
        part_of = total[base:base + 4, col:col + BLOCK]
        mean = part_of[0:1]
        inv = lax.rsqrt(part_of[1:2] - mean * mean + norm_eps)
        first = part_of[2:3]
        second = inv * (part_of[3:4] - mean * first)

        def spread(row):
            return jnp.broadcast_to(row, (BLOCK, BLOCK)).T

        inv_w = spread(inv)
        centred = (gat[rows, :] - spread(mean)) * inv_w
        normed = (centred * gain).astype(bf16)
        mixed = dot(spatial, normed, 1, 0) + bias
        joined[rows, 0:BLOCK] = (cs[rows, :] * mixed).astype(bf16)
        back = inv_w * (cg[rows, :] - spread(first) - centred * spread(second))
        joined[rows, BLOCK:2 * BLOCK] = (back * slope_g[rows, :]).astype(bf16)
        mixing = mixing + dot(mg[rows, :], normed, 1, 1)
    mixing = jnp.where(keep, mixing, 0.0)

    waits = stat_copies

    order = [(slot, h) for slot in range(nz) for h in range(2)]
    pieces_in = len(order)

    def input_part(n):
        slot, h = order[n]
        grads = joined[pl.ds(h * half, half), :]
        at = pl.multiple_of(z_xor[3 - slot] * (4 * BLOCK), 4 * BLOCK)
        res = dot(grads, wts[pl.ds(at, 4 * BLOCK), :], 1, 1).astype(bf16)
        for yy in range(2):
            for cc in range(2):
                at = (yy * 2 + cc) * BLOCK
                part[n, cc, yy] = res[:, at:at + BLOCK]
        copy = remote(part.at[n, 1 - c], r_core.at[n], core_send.at[n], core_recv.at[n], dev(i, j_core))
        copy.start()
        waits.append(copy)
        core_copies[n] = copy

    def weight_part(t):
        at = pl.multiple_of(theirs + t * tile, tile)
        gs[t] = dot(hid_t[pl.ds(at, tile), :], joined[...], 1, 0).astype(bf16)
        copy = remote(gs.at[t], gr.at[t], gx_send.at[t], gx_recv.at[t], dev(x_peer, j))
        copy.start()
        waits.append(copy)
        return copy

    core_copies, y_copies, z_copies, g_copies = {}, {}, {}, {}

    def second_stage(n):
        core_copies[n].wait_recv()
        q_send[n] = (part[n, c, 1 - y].astype(f32) + r_core[n, 1 - y].astype(f32)).astype(bf16)
        copy = remote(q_send.at[n], r_y.at[n], y_send.at[n], y_recv.at[n], dev(i, j_y))
        copy.start()
        waits.append(copy)
        y_copies[n] = copy

    def direct(h):
        return remote(z_send.at[0, h], r_z.at[0, h], zz_send.at[0, h], zz_recv.at[0, h], dev(i, z_dev(3)))

    def relay(h):
        return remote(z_send.at[0, h], r_z.at[3, h], zz_send.at[0, h], zz_recv.at[3, h], dev(i, z_dev(1)))

    def third_stage(n):
        slot, h = order[n]
        y_copies[n].wait_recv()
        res = (part[n, c, y].astype(f32) + r_core[n, y].astype(f32)) + r_y[n].astype(f32)
        if slot == nz - 1:
            acc[h] = res
            return
        if slot == 0:
            z_send[0, h] = res.astype(bf16)

            @pl.when(mid == 1)
            def _():
                direct(h).start()

            @pl.when(mid == 0)
            def _():
                relay(h).start()

            waits.append(direct(h))
            return
        if slot == 1:

            @pl.when(mid == 1)
            def _():
                relay(h).wait_recv()
                z_send[1, h] = (res + r_z[3, h].astype(f32)).astype(bf16)

            @pl.when(mid == 0)
            def _():
                z_send[1, h] = res.astype(bf16)
        else:
            z_send[slot, h] = res.astype(bf16)
        copy = remote(
            z_send.at[slot, h], r_z.at[slot, h], zz_send.at[slot, h], zz_recv.at[slot, h], dev(i, z_dev(3 - slot))
        )
        copy.start()
        waits.append(copy)
        z_copies[slot, h] = copy

    def last_stage(h):
        @pl.when(mid == 1)
        def _():
            direct(h).wait_recv()
            acc[h] = acc[h] + r_z[0, h].astype(f32)

        res = acc[h]
        for slot in range(1, nz - 1):
            z_copies[slot, h].wait_recv()
            res = res + r_z[slot, h].astype(f32)
        x_out[pl.ds(h * half, half), :] = res.astype(bf16)

    for step in range(pieces_in + 2):
        if step < pieces_in:
            input_part(step)
        if step < tiles:
            g_copies[step] = weight_part(step)
        if step >= 2:
            second_stage(step - 2)
    ms[...] = mixing.astype(bf16)
    m_copy = remote(ms, mr, mx_send, mx_recv, dev(x_peer, j))
    m_copy.start()
    waits.append(m_copy)
    for t in range(tiles):
        at = pl.multiple_of(mine + t * tile, tile)
        go[pl.ds(t * tile, tile), :] = dot(hid_t[pl.ds(at, tile), :], joined[...], 1, 0)
    for n in range(pieces_in):
        third_stage(n)
    for t in range(tiles):
        g_copies[t].wait_recv()
        rows = pl.ds(t * tile, tile)
        done = (go[rows, :] + gr[t].astype(f32)) * grad_scale
        c_out[rows, :] = done[:, 0:BLOCK]
        g_out[rows, :] = done[:, BLOCK:2 * BLOCK]
    m_copy.wait_recv()
    m_out[0] = (mixing + mr[...].astype(f32)) * grad_scale
    for h in range(2):
        last_stage(h)
    for copy in w_copies + waits:
        copy.wait_send()


def store_kernel(*refs):
    count = len(refs) // 2
    src, dst, sem = refs[:count], refs[count:2 * count], refs[-1]
    stores = [pltpu.make_async_copy(src[k], dst[k], sem.at[k]) for k in range(count)]
    for store in stores:
        store.start()
    for store in stores:
        store.wait()


def fused(n_dp, hidden_in, content_weight, gating_weight, norm_gain, mixing_weight, mixing_bias, out_grad):
    toks, depth = hidden_in.shape
    shard, width = content_weight.shape
    half = toks // 2
    nz = n_dp // 4
    tile = 256
    tiles = shard // tile
    pieces = 2
    grad_scale = 1.0 / math.sqrt(2 * toks)
    bf16, f32 = jnp.bfloat16, jnp.float32
    in_hbm = pl.BlockSpec(memory_space=pltpu.HBM)
    dma = pltpu.SemaphoreType.DMA
    V = pltpu.VMEM
    scratch = [
        V((1, width), f32), V((1, BLOCK, BLOCK), bf16), V((1, BLOCK), f32),
        V((toks, depth), bf16), V((depth, toks), bf16), V((depth, 2 * width), bf16), V((toks, width), bf16),
        V((toks, width), f32), V((toks, width), f32), V((toks, width), f32), V((toks, width), f32),
        V((toks, width), f32), V((toks, width), bf16), V((toks, 2 * width), bf16),
        V((8, toks // 2), f32), V((n_dp - 1, 8, toks // 2), f32),
        V((2 * nz, 2, 2, half, width), bf16), V((2 * nz, 2, half, width), bf16),
        V((2 * nz, half, width), bf16), V((2 * nz, half, width), bf16),
        V((nz - 1, 2, half, width), bf16), V((nz, 2, half, width), bf16), V((2, half, width), f32),
        V((tiles, tile, 2 * width), bf16), V((tiles, tile, 2 * width), bf16), V((shard, 2 * width), f32),
        V((BLOCK, BLOCK), bf16), V((BLOCK, BLOCK), bf16),
        dma((7,)), dma((2 * pieces,)), dma((2 * pieces,)), dma((n_dp - 1,)), dma((n_dp - 1,)), pltpu.SemaphoreType.REGULAR,
        dma((2 * nz,)), dma((2 * nz,)), dma((2 * nz,)), dma((2 * nz,)), dma((nz - 1, 2)), dma((nz, 2)),
        dma((tiles,)), dma((tiles,)), dma, dma,
    ]
    results = pl.pallas_call(
        functools.partial(fused_kernel, n_dp, width * n_dp, grad_scale),
        out_shape=(
            V((toks, width), bf16),
            V((shard, width), f32),
            V((shard, width), f32),
            V(mixing_weight.shape, f32),
        ),
        in_specs=[in_hbm] * 7,
        out_specs=(pl.BlockSpec(memory_space=pltpu.VMEM),) * 4,
        scratch_shapes=scratch,
        compiler_params=pltpu.CompilerParams(
            collective_id=0, has_side_effects=True, vmem_limit_bytes=60*1024*1024
        ),
    )(hidden_in, content_weight, gating_weight, norm_gain[None, :], mixing_weight, mixing_bias, out_grad)
    return pl.pallas_call(
        store_kernel,
        out_shape=tuple(jax.ShapeDtypeStruct(r.shape, r.dtype) for r in results),
        in_specs=[pl.BlockSpec(memory_space=pltpu.VMEM)] * 4,
        out_specs=(in_hbm,) * 4,
        scratch_shapes=[dma((4,))],
    )(*[pltpu.with_memory_space_constraint(r, pltpu.VMEM) for r in results])


def fits(n_sp, n_dp, toks, shard, width):
    paired = n_sp == 2 and n_dp == 16
    return paired and width == GROUP_DIM and shard % 512 == 0 and toks % (2 * BLOCK) == 0 and toks <= shard


def solve(*args):
    n_sp, n_dp = lax.axis_size("sp"), lax.axis_size("dp")
    shard, width = args[1].shape
    if fits(n_sp, n_dp, args[0].shape[0], shard, width) and args[0].shape[1] == n_dp * width:
        return fused(n_dp, *args)
    return local(*args)


def solution(mesh):
    in_specs = (
        P("sp", None),
        P("sp", "dp"),
        P("sp", "dp"),
        P("dp"),
        P("dp", None, None),
        P("dp", None),
        P("sp", "dp"),
    )
    out_specs = (P("sp", "dp"), P("sp", "dp"), P("sp", "dp"), P("dp", None, None))
    return jax.shard_map(solve, mesh=mesh, in_specs=in_specs, out_specs=out_specs, check_vma=False)
```

```python
import functools
import math

import jax
import jax.numpy as jnp
from jax import lax
from jax.experimental import pallas as pl
from jax.experimental.pallas import tpu as pltpu
from jax.sharding import PartitionSpec as P

GROUP_DIM = 128
BLOCK = 128


norm_eps = 1e-05


def gelu_slope(values):
    cumulative = 0.5 * (1.0 + lax.erf(values * (1.0 / math.sqrt(2.0))))
    density = jnp.exp(-0.5 * values * values) * (1.0 / math.sqrt(2.0 * math.pi))
    return cumulative + values * density


def causal_table(weights):
    row_ids = lax.broadcasted_iota(jnp.int32, (BLOCK, BLOCK), 0)
    col_ids = lax.broadcasted_iota(jnp.int32, (BLOCK, BLOCK), 1)
    keeper = (col_ids <= row_ids)[None]
    return (jnp.where(keeper, weights, jnp.zeros_like(weights)), keeper)


def hidden_term(hidden_in, grads):
    return lax.dot_general(
        hidden_in, grads, (((0,), (0,)), ((), ())), preferred_element_type=jnp.float32
    )


def local(
    hidden_in, content_weight, gating_weight, norm_gain, mixing_weight, mixing_bias, out_grad
):
    tok_rows = hidden_in.shape[0]
    local_width = content_weight.shape[1]
    groups_here = local_width // GROUP_DIM
    blocks = tok_rows // BLOCK
    full_width = local_width * lax.axis_size("dp")
    grad_scale = 1.0 / math.sqrt(tok_rows * lax.axis_size("sp"))
    whole_content, whole_gating = (
        lax.all_gather(content_weight, "sp", axis=0, tiled=True),
        lax.all_gather(gating_weight, "sp", axis=0, tiled=True),
    )
    joined_weight = jnp.concatenate([whole_content, whole_gating], axis=1)
    pre_both = jnp.dot(hidden_in, joined_weight, preferred_element_type=jnp.float32).astype(
        jnp.bfloat16
    )
    pre_content = pre_both[:, :local_width].astype(jnp.float32)
    pre_gating = pre_both[:, local_width:].astype(jnp.float32)
    content = jax.nn.gelu(pre_content, approximate=False)
    gating = jax.nn.gelu(pre_gating, approximate=False)
    spatial, keeper = causal_table(mixing_weight)
    grad_wide = out_grad.astype(jnp.float32)
    mixed_grad = (grad_wide * content).astype(jnp.bfloat16)
    mixed_blocks = mixed_grad.reshape(blocks, BLOCK, groups_here, GROUP_DIM)
    normed_grad = jnp.einsum(
        "gts,btgc->bsgc", spatial, mixed_blocks, preferred_element_type=jnp.float32
    )
    centred_grad = normed_grad.reshape(tok_rows, local_width) * norm_gain[None, :]
    row_sum, row_square, grad_sum, grad_raw = lax.psum(
        (
            jnp.sum(gating, axis=1),
            jnp.sum(gating * gating, axis=1),
            jnp.sum(centred_grad, axis=1),
            jnp.sum(centred_grad * gating, axis=1),
        ),
        "dp",
    )
    row_mean = (row_sum / full_width)[:, None]
    row_var = (row_square / full_width)[:, None] - row_mean * row_mean
    inv_std = lax.rsqrt(row_var + norm_eps)
    centred = (gating - row_mean) * inv_std
    first_moment = (grad_sum / full_width)[:, None]
    second_moment = inv_std * ((grad_raw / full_width)[:, None] - row_mean * first_moment)
    normed = (centred * norm_gain[None, :]).astype(jnp.bfloat16)
    normed_blocks = normed.reshape(blocks, BLOCK, groups_here, GROUP_DIM)
    mixed = jnp.einsum("gts,bsgc->btgc", spatial, normed_blocks, preferred_element_type=jnp.float32)
    mixed = (mixed + jnp.transpose(mixing_bias)[None, :, :, None]).reshape(tok_rows, local_width)
    content_pre_grad = (grad_wide * mixed * gelu_slope(pre_content)).astype(jnp.bfloat16)
    local_mixing = jnp.einsum(
        "btgc,bsgc->gts", mixed_blocks, normed_blocks, preferred_element_type=jnp.float32
    )
    local_mixing = jnp.where(keeper, local_mixing, 0.0)
    mixing_grad = lax.psum(local_mixing.astype(jnp.bfloat16), "sp").astype(jnp.float32) * grad_scale
    gating_back = inv_std * (centred_grad - first_moment - centred * second_moment)
    gating_pre_grad = (gating_back * gelu_slope(pre_gating)).astype(jnp.bfloat16)
    joined_grad = jnp.concatenate([content_pre_grad, gating_pre_grad], axis=1)
    partial_input = lax.dot_general(
        joined_grad, joined_weight, (((1,), (1,)), ((), ())), preferred_element_type=jnp.float32
    )
    input_grad = lax.psum_scatter(
        partial_input.astype(jnp.bfloat16), "dp", scatter_dimension=1, tiled=True
    )
    both_grads = (
        lax.psum_scatter(
            hidden_term(hidden_in, joined_grad).astype(jnp.bfloat16),
            "sp",
            scatter_dimension=0,
            tiled=True,
        ).astype(jnp.float32)
        * grad_scale
    )
    content_grad = both_grads[:, :local_width]
    gating_grad = both_grads[:, local_width:]
    return (input_grad, content_grad, gating_grad, mixing_grad)


def phi_and_slope(values):
    cumulative = 0.5 * (1.0 + lax.erf(values * (1.0 / math.sqrt(2.0))))
    density = jnp.exp(-0.5 * values * values) * (1.0 / math.sqrt(2.0 * math.pi))
    return cumulative, cumulative + values * density


def dot(a, b, ca, cb):
    return lax.dot_general(
        a, b, (((ca,), (cb,)), ((), ())), preferred_element_type=jnp.float32
    )


def fused_kernel(
    n_dp, full_width, grad_scale,
    h_in, wc_in, wg_in, gain_in, mix_in, bias_in, og_in,
    x_out, c_out, g_out, m_out,
    gain_ref, mix_ref, bias_ref, hid, hid_t, wts, wq, og, pre_acc,
    cs, gat, gat_t, slope_g, mg, cg, centred_ref, eq, part,
    s1, r1, s2, r2, z_send, r_z, gs, gr,
    load_sem, hello, quad_ok, all_ok, w_send, w_recv, q_send, q_recv, a_send, a_recv,
    e_send, c_recv, yg_recv, sg_recv, gx_send, gx_recv, zz_send, zz_recv, relay_recv,
):
    toks = hid.shape[0]
    chunks = toks // BLOCK
    nz = n_dp // 4
    zs = nz // 2
    shard = zs * 4 * BLOCK
    tile = shard // chunks
    bf16 = jnp.bfloat16
    f32 = jnp.float32

    i = lax.axis_index("sp")
    j = lax.axis_index("dp")
    x_peer = 1 - i
    c = lax.rem(j, 2)
    y = lax.rem(j // 2, 2)
    z = j // 4
    me = y * 2 + c
    y_mate = (1 - y) * 2 + c
    mates = (y * 2 + 1 - c, y_mate, (1 - y) * 2 + 1 - c)

    mid = lax.rem((z + 1) // 2, 2)
    z_xor = (z, z + 1 - 2 * lax.rem(z, 2), z + 2 - 4 * (z // 2), 3 - z)

    def dev(a, b):
        return {"sp": a, "dp": b}

    def mate_dev(rel):
        return dev(i, z * 4 + mates[rel])

    def z_dev(q):
        return dev(i, z_xor[q] * 4 + me)

    def remote(src, dst, ssem, rsem, target):
        return pltpu.make_async_remote_copy(
            src_ref=src, dst_ref=dst, send_sem=ssem, recv_sem=rsem,
            device_id=target, device_id_type=pl.DeviceIdType.MESH,
        )

    def send(*args):
        remote(*args).start()

    def await_bytes(ref, sem):
        pltpu.make_async_copy(ref, ref, sem).wait()

    def tell(sem, target):
        pl.semaphore_signal(sem, inc=1, device_id=target, device_id_type=pl.DeviceIdType.MESH)

    x_dev = dev(x_peer, j)
    my_z = pl.ds(zs * i, zs)
    their_z = pl.ds(zs * x_peer, zs)
    mine = pl.multiple_of(i * shard, shard)
    theirs = pl.multiple_of(x_peer * shard, shard)
    loads = [
        pltpu.make_async_copy(wg_in, wts.at[1, my_z], load_sem.at[0]),
        pltpu.make_async_copy(wc_in, wts.at[0, my_z], load_sem.at[1]),
        pltpu.make_async_copy(h_in, hid, load_sem.at[2]),
        pltpu.make_async_copy(og_in, og, load_sem.at[3]),
        pltpu.make_async_copy(gain_in, gain_ref, load_sem.at[4]),
        pltpu.make_async_copy(mix_in, mix_ref, load_sem.at[5]),
        pltpu.make_async_copy(bias_in, bias_ref, load_sem.at[6]),
    ]
    for load in loads:
        load.start()

    barrier = pltpu.get_barrier_semaphore()
    lead = i == 0
    follow = i == 1
    herald = jnp.logical_and(lead, me == 1)
    plain = jnp.logical_and(lead, me != 1)

    @pl.when(lead)
    def _():
        tell(barrier, x_dev)

    @pl.when(follow)
    def _():
        pl.semaphore_wait(barrier, 1)
        tell(hello, x_dev)

    @pl.when(lead)
    def _():
        pl.semaphore_wait(hello, 1)

    half_at = (pl.multiple_of((1 - y) * 2 * BLOCK, 2 * BLOCK), pl.multiple_of(y * 2 * BLOCK, 2 * BLOCK))

    def w_copy(which, own):
        ref = wts.at[which, my_z, pl.ds(half_at[own], 2 * BLOCK)]
        return remote(ref, ref, w_send, w_recv.at[which, own], x_dev)

    for which in (1, 0):
        loads[1 - which].wait()
        for own in range(2):
            w_copy(which, own).start()

    for rel in range(3):

        @pl.when(jnp.logical_and(lead, mates[rel] != 1))
        def _():
            tell(barrier, mate_dev(rel))

    @pl.when(plain)
    def _():
        pl.semaphore_wait(barrier, 3)
        tell(quad_ok, dev(i, z * 4 + 1))
        tell(hello, x_dev)

    @pl.when(herald)
    def _():
        pl.semaphore_wait(quad_ok, 3)
        tell(hello, x_dev)
        for q in range(1, nz):
            tell(barrier, z_dev(q))

    @pl.when(follow)
    def _():
        pl.semaphore_wait(hello, 1)

    others = [dev(i, lax.rem(j + k, n_dp)) for k in range(1, n_dp)]

    def hand_on(which, part_z, rel):
        at = pl.multiple_of(mates[rel] * BLOCK, BLOCK)
        send(wts.at[which, part_z, pl.ds(at, BLOCK)], wq.at[which, me, part_z], q_send, q_recv, mate_dev(rel))

    def keep_own(which, part_z):
        at = pl.multiple_of(me * BLOCK, BLOCK)
        wq[which, me, part_z] = wts[which, part_z, pl.ds(at, BLOCK)]

    for which in (1, 0):
        for rel in (1, 2, 0):
            hand_on(which, my_z, rel)

    keep = lax.broadcasted_iota(jnp.int32, (BLOCK, BLOCK), 1) <= lax.broadcasted_iota(
        jnp.int32, (BLOCK, BLOCK), 0
    )
    for load in loads[2:]:
        load.wait()
    spatial = jnp.where(keep, mix_ref[0].astype(f32), 0.0).astype(bf16)
    gain = gain_ref[...]
    bias = jnp.broadcast_to(bias_ref[...], (BLOCK, BLOCK)).T
    both = jnp.concatenate([wts[which, my_z].reshape(shard, BLOCK) for which in range(2)], axis=1)
    own = dot(hid[:, pl.ds(mine, shard)], both, 1, 0)
    pre_acc[0] = own[:, 0:BLOCK]
    pre_acc[1] = own[:, BLOCK:2 * BLOCK]
    for b in range(hid.shape[1] // BLOCK):
        hid_t[pl.ds(b * BLOCK, BLOCK), :] = hid[:, pl.ds(b * BLOCK, BLOCK)].T
    for which in range(2):
        keep_own(which, my_z)

    def finish(which, own):
        w_copy(which, own).wait_recv()
        part_sum = pre_acc[which]
        for zz in range(zs):
            at = pl.multiple_of(theirs + zz * 4 * BLOCK + half_at[own], 2 * BLOCK)
            part_sum = part_sum + dot(
                hid[:, pl.ds(at, 2 * BLOCK)],
                wts[which, zs * x_peer + zz, pl.ds(half_at[own], 2 * BLOCK)], 1, 0,
            )
        pre_acc[which] = part_sum

    def share(n, src, dst):
        for k, target in enumerate(others):
            send(src, dst.at[k], a_send.at[n], a_recv.at[n], target)

    def gather(n, src, dst):
        await_bytes(dst, a_recv.at[n])
        total = src[...]
        for k in range(len(others)):
            total = total + dst[k]
        return total * (1.0 / full_width)

    finish(1, 0)
    for rel in (1, 2):
        hand_on(1, their_z, rel)
    finish(1, 1)
    for k in range(chunks):
        rows = pl.ds(k * BLOCK, BLOCK)
        pre = pre_acc[1, rows, :].astype(bf16).astype(f32)
        cumulative, slope = phi_and_slope(pre)
        gating = pre * cumulative
        gat[rows, :] = gating
        slope_g[rows, :] = slope
        turned = gating.T
        gat_t[rows, :] = turned
        s1[k:k + 1, :] = jnp.sum(turned, axis=0, keepdims=True)
        s1[chunks + k:chunks + k + 1, :] = jnp.sum(turned * turned, axis=0, keepdims=True)

    @pl.when(herald)
    def _():
        pl.semaphore_wait(barrier, nz - 1)
        for rel in range(3):
            tell(all_ok, mate_dev(rel))
            tell(all_ok, dev(x_peer, z * 4 + mates[rel]))
        tell(all_ok, x_dev)

    @pl.when(jnp.logical_not(herald))
    def _():
        pl.semaphore_wait(all_ok, 1)

    share(0, s1, r1)
    hand_on(1, their_z, 0)
    keep_own(1, their_z)

    finish(0, 0)
    for rel in (1, 2):
        hand_on(0, their_z, rel)
    finish(0, 1)
    for k in range(chunks):
        rows = pl.ds(k * BLOCK, BLOCK)
        pre = pre_acc[0, rows, :].astype(bf16).astype(f32)
        wide = og[rows, :].astype(f32)
        cumulative, slope = phi_and_slope(pre)
        cs[rows, :] = wide * slope
        mixed_grad = (wide * (pre * cumulative)).astype(bf16)
        mg[rows, :] = mixed_grad
        centred_grad = dot(spatial, mixed_grad, 0, 0) * gain
        cg[rows, :] = centred_grad
        turned = centred_grad.T
        s2[k:k + 1, :] = jnp.sum(turned, axis=0, keepdims=True)
        s2[chunks + k:chunks + k + 1, :] = jnp.sum(turned * gat_t[rows, :], axis=0, keepdims=True)
    share(1, s2, r2)
    hand_on(0, their_z, 0)
    keep_own(0, their_z)

    def spread(row):
        return jnp.broadcast_to(row, (BLOCK, BLOCK)).T

    def exchange(which, k):
        ref = eq.at[which, me, pl.ds(k * BLOCK, BLOCK)]
        y_sem = yg_recv.at[k] if which else c_recv.at[0]
        s_sem = sg_recv.at[k] if which else c_recv.at[1]
        send(ref, ref, e_send, y_sem, mate_dev(1))
        send(ref, ref, e_send, s_sem, mate_dev(0))

    def all_terms(which, k):
        rows = pl.ds(k * BLOCK, BLOCK)
        grads = jnp.concatenate([eq[which, q, rows, :] for q in range(4)], axis=1)
        weights = jnp.concatenate([wq[which, q].reshape(nz * BLOCK, BLOCK) for q in range(4)], axis=1)
        return dot(grads, weights, 1, 1)

    t1 = gather(0, s1, r1)
    means, invs = [], []
    mixing = jnp.zeros((BLOCK, BLOCK), f32)
    for k in range(chunks):
        rows = pl.ds(k * BLOCK, BLOCK)
        mean = t1[k:k + 1]
        inv = lax.rsqrt(t1[chunks + k:chunks + k + 1] - mean * mean + norm_eps)
        means.append(mean)
        invs.append(inv)
        inv_w = spread(inv)
        centred = (gat[rows, :] - spread(mean)) * inv_w
        centred_ref[rows, :] = centred
        slope_g[rows, :] = slope_g[rows, :] * inv_w
        normed = (centred * gain).astype(bf16)
        mixed = dot(spatial, normed, 1, 0) + bias
        eq[0, me, rows, :] = (cs[rows, :] * mixed).astype(bf16)
        exchange(0, k)
        mixing = mixing + dot(mg[rows, :], normed, 1, 1)
    mixing = jnp.where(keep, mixing, 0.0)

    def weight_part(which, t):
        at = pl.multiple_of(theirs + t * tile, tile)
        rows = pl.ds(t * tile, tile)
        gs[which, rows, :] = dot(hid_t[pl.ds(at, tile), :], eq[which, me], 1, 0).astype(bf16)
        send(gs.at[which, rows], gr.at[which, rows], gx_send.at[which], gx_recv.at[which], x_dev)

    outs = (c_out, g_out)

    def weight_own(which, t):
        at = pl.multiple_of(mine + t * tile, tile)
        outs[which][pl.ds(t * tile, tile), :] = dot(hid_t[pl.ds(at, tile), :], eq[which, me], 1, 0)

    last = pl.ds(shard, BLOCK)
    gs[0, last, :] = mixing.astype(bf16)
    send(gs.at[0, last], gr.at[0, last], gx_send.at[0], gx_recv.at[0], x_dev)
    for t in range(chunks):
        weight_part(0, t)
    for t in range(chunks):
        weight_own(0, t)

    t2 = gather(1, s2, r2)
    for k in range(chunks):
        rows = pl.ds(k * BLOCK, BLOCK)
        first = t2[k:k + 1]
        second = invs[k] * (t2[chunks + k:chunks + k + 1] - means[k] * first)
        back = cg[rows, :] - spread(first) - centred_ref[rows, :] * spread(second)
        eq[1, me, rows, :] = (back * slope_g[rows, :]).astype(bf16)
        exchange(1, k)
    await_bytes(eq.at[0, 0], c_recv.at[0])
    handed = eq.at[0, y_mate]
    send(handed, handed, e_send, c_recv.at[1], mate_dev(0))
    await_bytes(wq.at[:, pl.ds(0, 3)], q_recv)
    await_bytes(eq.at[0, pl.ds(0, 2)], c_recv.at[1])
    for k in range(chunks):
        res = all_terms(0, k)
        for q in range(nz):
            part[k, q] = res[:, q * BLOCK:(q + 1) * BLOCK]

    def z_go(slot, k, rsem, land, q):
        send(z_send.at[slot, k], r_z.at[land, k], zz_send, rsem, z_dev(q))

    def pass_on(k):
        rows = pl.ds(k * BLOCK, BLOCK)
        await_bytes(eq.at[1, 0, rows], yg_recv.at[k])
        ref = eq.at[1, y_mate, rows]
        send(ref, ref, e_send, sg_recv.at[k], mate_dev(0))

    def spread_out(k):
        await_bytes(eq.at[1, pl.ds(0, 2), pl.ds(k * BLOCK, BLOCK)], sg_recv.at[k])
        res = all_terms(1, k)
        for q in range(nz):
            part[k, q] = part[k, q] + res[:, q * BLOCK:(q + 1) * BLOCK]
        z_send[0, k] = part[k, z_xor[3]].astype(bf16)

        @pl.when(mid == 0)
        def _():
            z_go(0, k, relay_recv.at[k], 3, 1)

        @pl.when(mid == 1)
        def _():
            z_go(0, k, zz_recv.at[0], 0, 3)
            z_send[2, k] = part[k, z_xor[1]].astype(bf16)
            z_go(2, k, zz_recv.at[1], 2, 1)

    def relay(k):
        @pl.when(mid == 1)
        def _():
            await_bytes(r_z.at[3, k], relay_recv.at[k])
            z_send[1, k] = (part[k, z_xor[2]] + r_z[3, k].astype(f32)).astype(bf16)
            z_go(1, k, zz_recv.at[1], 1, 2)

        @pl.when(mid == 0)
        def _():
            z_send[1, k] = part[k, z_xor[2]].astype(bf16)
            z_go(1, k, zz_recv.at[1], 1, 2)
            z_send[2, k] = part[k, z_xor[1]].astype(bf16)
            z_go(2, k, zz_recv.at[1], 2, 1)

    for step in range(chunks + 1):
        if step < chunks:
            pass_on(step)
        if step >= 1:
            spread_out(step - 1)
            weight_part(1, step - 1)
    for k in range(chunks):
        relay(k)
        weight_own(1, k)

    for which in range(2):
        rows = pl.ds(0, shard + (1 - which) * BLOCK)
        await_bytes(gr.at[which, rows], gx_recv.at[which])
        for t in range(chunks):
            rows = pl.ds(t * tile, tile)
            outs[which][rows, :] = (outs[which][rows, :] + gr[which, rows, :].astype(f32)) * grad_scale
        if which == 0:
            m_out[0] = (mixing + gr[0, last, :].astype(f32)) * grad_scale

    @pl.when(mid == 1)
    def _():
        await_bytes(r_z.at[0], zz_recv.at[0])
        for k in range(chunks):
            part[k, z] = part[k, z] + r_z[0, k].astype(f32)

    await_bytes(r_z.at[pl.ds(1, 2)], zz_recv.at[1])
    for k in range(chunks):
        x_out[pl.ds(k * BLOCK, BLOCK), :] = (
            part[k, z] + r_z[1, k].astype(f32) + r_z[2, k].astype(f32)
        ).astype(bf16)
    await_bytes(wts.at[:, my_z], w_send)
    await_bytes(wq.at[:, pl.ds(0, 3)], q_send)
    await_bytes(r1, a_send.at[0])
    await_bytes(r2, a_send.at[1])
    await_bytes(eq.at[:, pl.ds(0, 3)], e_send)
    await_bytes(gs.at[0], gx_send.at[0])
    await_bytes(gs.at[1, pl.ds(0, shard)], gx_send.at[1])
    await_bytes(z_send, zz_send)


def store_kernel(*refs):
    count = len(refs) // 2
    src, dst, sem = refs[:count], refs[count:2 * count], refs[-1]
    stores = [pltpu.make_async_copy(src[k], dst[k], sem.at[k]) for k in range(count)]
    for store in stores:
        store.start()
    for store in stores:
        store.wait()


def fused(n_dp, hidden_in, content_weight, gating_weight, norm_gain, mixing_weight, mixing_bias, out_grad):
    toks, depth = hidden_in.shape
    shard, width = content_weight.shape
    nz = n_dp // 4
    zs = nz // 2
    chunks = toks // BLOCK
    grad_scale = 1.0 / math.sqrt(2 * toks)
    bf16, f32 = jnp.bfloat16, jnp.float32
    in_hbm = pl.BlockSpec(memory_space=pltpu.HBM)
    dma = pltpu.SemaphoreType.DMA
    once = pltpu.SemaphoreType.REGULAR
    V = pltpu.VMEM
    wide = V((toks, width), f32)
    sums = V((2 * chunks, BLOCK), f32)
    sums_in = V((n_dp - 1, 2 * chunks, BLOCK), f32)
    scratch = [
        V((1, width), f32), V((1, BLOCK, BLOCK), bf16), V((1, BLOCK), f32),
        V((toks, depth), bf16), V((depth, toks), bf16), V((2, nz, 4 * BLOCK, width), bf16),
        V((2, 4, nz, BLOCK, width), bf16), V((toks, width), bf16), V((2, toks, width), f32),
        wide, wide, wide, wide, V((toks, width), bf16), wide, wide,
        V((2, 4, toks, width), bf16), V((chunks, nz, BLOCK, width), f32),
        sums, sums_in, sums, sums_in,
        V((nz - 1, chunks, BLOCK, width), bf16), V((nz, chunks, BLOCK, width), bf16),
        V((2, shard + BLOCK, width), bf16), V((2, shard + BLOCK, width), bf16),
        dma((7,)), once, once, once, dma, dma((2, 2)), dma, dma, dma((2,)), dma((2,)),
        dma, dma((2,)), dma((chunks,)), dma((chunks,)), dma((2,)), dma((2,)), dma, dma((2,)), dma((chunks,)),
    ]
    in_vmem = pl.BlockSpec(memory_space=V)
    results = pl.pallas_call(
        functools.partial(fused_kernel, n_dp, width * n_dp, grad_scale),
        out_shape=(
            V((toks, width), bf16),
            V((shard, width), f32),
            V((shard, width), f32),
            V(mixing_weight.shape, f32),
        ),
        in_specs=[in_hbm] * 7,
        out_specs=(in_vmem,) * 4,
        scratch_shapes=scratch,
        compiler_params=pltpu.CompilerParams(
            collective_id=0, has_side_effects=True, vmem_limit_bytes=60 * 1024 * 1024
        ),
    )(
        hidden_in, content_weight.reshape(zs, 4 * BLOCK, width), gating_weight.reshape(zs, 4 * BLOCK, width),
        norm_gain[None, :], mixing_weight, mixing_bias, out_grad,
    )
    return pl.pallas_call(
        store_kernel,
        out_shape=tuple(jax.ShapeDtypeStruct(r.shape, r.dtype) for r in results),
        in_specs=[in_vmem] * 4,
        out_specs=(in_hbm,) * 4,
        scratch_shapes=[dma((4,))],
        compiler_params=pltpu.CompilerParams(vmem_limit_bytes=60 * 1024 * 1024),
    )(*[pltpu.with_memory_space_constraint(r, V) for r in results])


def fits(n_sp, n_dp, toks, shard, width):
    paired = n_sp == 2 and n_dp == 16
    return paired and width == GROUP_DIM and shard == 2 * 4 * BLOCK and toks == 4 * BLOCK


def solve(*args):
    n_sp, n_dp = lax.axis_size("sp"), lax.axis_size("dp")
    shard, width = args[1].shape
    if fits(n_sp, n_dp, args[0].shape[0], shard, width) and args[0].shape[1] == n_dp * width:
        return fused(n_dp, *args)
    return local(*args)


def solution(mesh):
    in_specs = (
        P("sp", None),
        P("sp", "dp"),
        P("sp", "dp"),
        P("dp"),
        P("dp", None, None),
        P("dp", None),
        P("sp", "dp"),
    )
    out_specs = (P("sp", "dp"), P("sp", "dp"), P("sp", "dp"), P("dp", None, None))
    return jax.shard_map(solve, mesh=mesh, in_specs=in_specs, out_specs=out_specs, check_vma=False)
```

```python
import functools
import math

import jax
import jax.numpy as jnp
from jax import lax
from jax.experimental import pallas as pl
from jax.experimental.pallas import tpu as pltpu
from jax.sharding import PartitionSpec as P

GROUP_DIM = 128
BLOCK = 128


norm_eps = 1e-05


def gelu_slope(values):
    cumulative = 0.5 * (1.0 + lax.erf(values * (1.0 / math.sqrt(2.0))))
    density = jnp.exp(-0.5 * values * values) * (1.0 / math.sqrt(2.0 * math.pi))
    return cumulative + values * density


def causal_table(weights):
    row_ids = lax.broadcasted_iota(jnp.int32, (BLOCK, BLOCK), 0)
    col_ids = lax.broadcasted_iota(jnp.int32, (BLOCK, BLOCK), 1)
    keeper = (col_ids <= row_ids)[None]
    return (jnp.where(keeper, weights, jnp.zeros_like(weights)), keeper)


def hidden_term(hidden_in, grads):
    return lax.dot_general(
        hidden_in, grads, (((0,), (0,)), ((), ())), preferred_element_type=jnp.float32
    )


def local(
    hidden_in, content_weight, gating_weight, norm_gain, mixing_weight, mixing_bias, out_grad
):
    tok_rows = hidden_in.shape[0]
    local_width = content_weight.shape[1]
    groups_here = local_width // GROUP_DIM
    blocks = tok_rows // BLOCK
    full_width = local_width * lax.axis_size("dp")
    grad_scale = 1.0 / math.sqrt(tok_rows * lax.axis_size("sp"))
    whole_content, whole_gating = (
        lax.all_gather(content_weight, "sp", axis=0, tiled=True),
        lax.all_gather(gating_weight, "sp", axis=0, tiled=True),
    )
    joined_weight = jnp.concatenate([whole_content, whole_gating], axis=1)
    pre_both = jnp.dot(hidden_in, joined_weight, preferred_element_type=jnp.float32).astype(
        jnp.bfloat16
    )
    pre_content = pre_both[:, :local_width].astype(jnp.float32)
    pre_gating = pre_both[:, local_width:].astype(jnp.float32)
    content = jax.nn.gelu(pre_content, approximate=False)
    gating = jax.nn.gelu(pre_gating, approximate=False)
    spatial, keeper = causal_table(mixing_weight)
    grad_wide = out_grad.astype(jnp.float32)
    mixed_grad = (grad_wide * content).astype(jnp.bfloat16)
    mixed_blocks = mixed_grad.reshape(blocks, BLOCK, groups_here, GROUP_DIM)
    normed_grad = jnp.einsum(
        "gts,btgc->bsgc", spatial, mixed_blocks, preferred_element_type=jnp.float32
    )
    centred_grad = normed_grad.reshape(tok_rows, local_width) * norm_gain[None, :]
    row_sum, row_square, grad_sum, grad_raw = lax.psum(
        (
            jnp.sum(gating, axis=1),
            jnp.sum(gating * gating, axis=1),
            jnp.sum(centred_grad, axis=1),
            jnp.sum(centred_grad * gating, axis=1),
        ),
        "dp",
    )
    row_mean = (row_sum / full_width)[:, None]
    row_var = (row_square / full_width)[:, None] - row_mean * row_mean
    inv_std = lax.rsqrt(row_var + norm_eps)
    centred = (gating - row_mean) * inv_std
    first_moment = (grad_sum / full_width)[:, None]
    second_moment = inv_std * ((grad_raw / full_width)[:, None] - row_mean * first_moment)
    normed = (centred * norm_gain[None, :]).astype(jnp.bfloat16)
    normed_blocks = normed.reshape(blocks, BLOCK, groups_here, GROUP_DIM)
    mixed = jnp.einsum("gts,bsgc->btgc", spatial, normed_blocks, preferred_element_type=jnp.float32)
    mixed = (mixed + jnp.transpose(mixing_bias)[None, :, :, None]).reshape(tok_rows, local_width)
    content_pre_grad = (grad_wide * mixed * gelu_slope(pre_content)).astype(jnp.bfloat16)
    local_mixing = jnp.einsum(
        "btgc,bsgc->gts", mixed_blocks, normed_blocks, preferred_element_type=jnp.float32
    )
    local_mixing = jnp.where(keeper, local_mixing, 0.0)
    mixing_grad = lax.psum(local_mixing.astype(jnp.bfloat16), "sp").astype(jnp.float32) * grad_scale
    gating_back = inv_std * (centred_grad - first_moment - centred * second_moment)
    gating_pre_grad = (gating_back * gelu_slope(pre_gating)).astype(jnp.bfloat16)
    joined_grad = jnp.concatenate([content_pre_grad, gating_pre_grad], axis=1)
    partial_input = lax.dot_general(
        joined_grad, joined_weight, (((1,), (1,)), ((), ())), preferred_element_type=jnp.float32
    )
    input_grad = lax.psum_scatter(
        partial_input.astype(jnp.bfloat16), "dp", scatter_dimension=1, tiled=True
    )
    both_grads = (
        lax.psum_scatter(
            hidden_term(hidden_in, joined_grad).astype(jnp.bfloat16),
            "sp",
            scatter_dimension=0,
            tiled=True,
        ).astype(jnp.float32)
        * grad_scale
    )
    content_grad = both_grads[:, :local_width]
    gating_grad = both_grads[:, local_width:]
    return (input_grad, content_grad, gating_grad, mixing_grad)


def phi_and_slope(values):
    cumulative = 0.5 * (1.0 + lax.erf(values * (1.0 / math.sqrt(2.0))))
    density = jnp.exp(-0.5 * values * values) * (1.0 / math.sqrt(2.0 * math.pi))
    return cumulative, cumulative + values * density


def dot(a, b, ca, cb):
    return lax.dot_general(
        a, b, (((ca,), (cb,)), ((), ())), preferred_element_type=jnp.float32
    )


def fused_kernel(
    n_dp, full_width, grad_scale,
    h_in, wc_in, wg_in, gain_in, mix_in, bias_in, og_in,
    x_out, c_out, g_out, m_out,
    gain_ref, mix_ref, bias_ref, hid, hid_t, wts, wq, og, pre_acc,
    cs, gat, gat_t, slope_g, mg, cg, centred_ref, eq, part,
    s1, r1, s2, r2, z_send, r_z, gs, gr,
    load_sem, hello, quad_ok, all_ok, w_send, w_recv, q_send, q_recv, a_send, a_recv,
    e_send, c_recv, yg_recv, sg_recv, gx_send, gx_recv, zz_send, zz_recv, relay_recv,
):
    toks = hid.shape[0]
    chunks = toks // BLOCK
    nz = n_dp // 4
    zs = nz // 2
    shard = zs * 4 * BLOCK
    tile = shard // chunks
    bf16 = jnp.bfloat16
    f32 = jnp.float32

    i = lax.axis_index("sp")
    j = lax.axis_index("dp")
    x_peer = 1 - i
    c = lax.rem(j, 2)
    y = lax.rem(j // 2, 2)
    z = j // 4
    me = y * 2 + c
    y_mate = (1 - y) * 2 + c
    mates = (y * 2 + 1 - c, y_mate, (1 - y) * 2 + 1 - c)

    mid = lax.rem((z + 1) // 2, 2)
    z_xor = (z, z + 1 - 2 * lax.rem(z, 2), z + 2 - 4 * (z // 2), 3 - z)

    def dev(a, b):
        return {"sp": a, "dp": b}

    def mate_dev(rel):
        return dev(i, z * 4 + mates[rel])

    def z_dev(q):
        return dev(i, z_xor[q] * 4 + me)

    def remote(src, dst, ssem, rsem, target):
        return pltpu.make_async_remote_copy(
            src_ref=src, dst_ref=dst, send_sem=ssem, recv_sem=rsem,
            device_id=target, device_id_type=pl.DeviceIdType.MESH,
        )

    def send(*args):
        remote(*args).start()

    def await_bytes(ref, sem):
        pltpu.make_async_copy(ref, ref, sem).wait()

    def tell(sem, target):
        pl.semaphore_signal(sem, inc=1, device_id=target, device_id_type=pl.DeviceIdType.MESH)

    x_dev = dev(x_peer, j)
    my_z = pl.ds(zs * i, zs)
    their_z = pl.ds(zs * x_peer, zs)
    mine = pl.multiple_of(i * shard, shard)
    theirs = pl.multiple_of(x_peer * shard, shard)
    loads = [
        pltpu.make_async_copy(wg_in, wts.at[1, my_z], load_sem.at[0]),
        pltpu.make_async_copy(wc_in, wts.at[0, my_z], load_sem.at[1]),
        pltpu.make_async_copy(h_in, hid, load_sem.at[2]),
        pltpu.make_async_copy(og_in, og, load_sem.at[3]),
        pltpu.make_async_copy(gain_in, gain_ref, load_sem.at[4]),
        pltpu.make_async_copy(mix_in, mix_ref, load_sem.at[5]),
        pltpu.make_async_copy(bias_in, bias_ref, load_sem.at[6]),
    ]
    for load in loads:
        load.start()

    barrier = pltpu.get_barrier_semaphore()
    lead = i == 0
    follow = i == 1
    herald = jnp.logical_and(lead, me == 1)
    plain = jnp.logical_and(lead, me != 1)

    @pl.when(lead)
    def _():
        tell(barrier, x_dev)

    @pl.when(follow)
    def _():
        pl.semaphore_wait(barrier, 1)
        tell(hello, x_dev)

    @pl.when(lead)
    def _():
        pl.semaphore_wait(hello, 1)

    half_at = (pl.multiple_of((1 - y) * 2 * BLOCK, 2 * BLOCK), pl.multiple_of(y * 2 * BLOCK, 2 * BLOCK))

    def w_copy(which, own):
        ref = wts.at[which, my_z, pl.ds(half_at[own], 2 * BLOCK)]
        return remote(ref, ref, w_send, w_recv.at[which, own], x_dev)

    for which in (1, 0):
        loads[1 - which].wait()
        w_copy(which, 0).start()
        if which == 1:
            w_copy(1, 1).start()

    @pl.when(c == 0)
    def _():
        w_copy(0, 1).start()

    for rel in range(3):

        @pl.when(jnp.logical_and(lead, mates[rel] != 1))
        def _():
            tell(barrier, mate_dev(rel))

    @pl.when(plain)
    def _():
        pl.semaphore_wait(barrier, 3)
        tell(quad_ok, dev(i, z * 4 + 1))
        tell(hello, x_dev)

    @pl.when(herald)
    def _():
        pl.semaphore_wait(quad_ok, 3)
        tell(hello, x_dev)
        for q in range(1, nz):
            tell(barrier, z_dev(q))

    @pl.when(follow)
    def _():
        pl.semaphore_wait(hello, 1)

    others = [dev(i, lax.rem(j + k, n_dp)) for k in range(1, n_dp)]

    def hand_on(which, part_z, rel):
        at = pl.multiple_of(mates[rel] * BLOCK, BLOCK)
        send(wts.at[which, part_z, pl.ds(at, BLOCK)], wq.at[which, me, part_z], q_send, q_recv, mate_dev(rel))

    def keep_own(which, part_z):
        at = pl.multiple_of(me * BLOCK, BLOCK)
        wq[which, me, part_z] = wts[which, part_z, pl.ds(at, BLOCK)]

    for which in (1, 0):
        for rel in (1, 2, 0):
            hand_on(which, my_z, rel)

    keep = lax.broadcasted_iota(jnp.int32, (BLOCK, BLOCK), 1) <= lax.broadcasted_iota(
        jnp.int32, (BLOCK, BLOCK), 0
    )
    for load in loads[2:]:
        load.wait()
    spatial = jnp.where(keep, mix_ref[0].astype(f32), 0.0).astype(bf16)
    gain = gain_ref[...]
    bias = jnp.broadcast_to(bias_ref[...], (BLOCK, BLOCK)).T
    both = jnp.concatenate([wts[which, my_z].reshape(shard, BLOCK) for which in range(2)], axis=1)
    own = dot(hid[:, pl.ds(mine, shard)], both, 1, 0)
    pre_acc[0] = own[:, 0:BLOCK]
    pre_acc[1] = own[:, BLOCK:2 * BLOCK]
    for b in range(hid.shape[1] // BLOCK):
        hid_t[pl.ds(b * BLOCK, BLOCK), :] = hid[:, pl.ds(b * BLOCK, BLOCK)].T
    for which in range(2):
        keep_own(which, my_z)

    def finish(which, own):
        w_copy(which, own).wait_recv()
        part_sum = pre_acc[which]
        for zz in range(zs):
            at = pl.multiple_of(theirs + zz * 4 * BLOCK + half_at[own], 2 * BLOCK)
            part_sum = part_sum + dot(
                hid[:, pl.ds(at, 2 * BLOCK)],
                wts[which, zs * x_peer + zz, pl.ds(half_at[own], 2 * BLOCK)], 1, 0,
            )
        pre_acc[which] = part_sum

    def share(n, src, dst):
        for k, target in enumerate(others):
            send(src, dst.at[k], a_send.at[n], a_recv.at[n], target)

    def gather(n, src, dst):
        await_bytes(dst, a_recv.at[n])
        total = src[...]
        for k in range(len(others)):
            total = total + dst[k]
        return total * (1.0 / full_width)

    finish(1, 0)
    for rel in (1, 2):
        hand_on(1, their_z, rel)
    finish(1, 1)

    @pl.when(c == 1)
    def _():
        w_copy(0, 1).start()

    for k in range(chunks):
        rows = pl.ds(k * BLOCK, BLOCK)
        pre = pre_acc[1, rows, :].astype(bf16).astype(f32)
        cumulative, slope = phi_and_slope(pre)
        gating = pre * cumulative
        gat[rows, :] = gating
        slope_g[rows, :] = slope
        turned = gating.T
        gat_t[rows, :] = turned
        s1[k:k + 1, :] = jnp.sum(turned, axis=0, keepdims=True)
        s1[chunks + k:chunks + k + 1, :] = jnp.sum(turned * turned, axis=0, keepdims=True)

    @pl.when(herald)
    def _():
        pl.semaphore_wait(barrier, nz - 1)
        for rel in range(3):
            tell(all_ok, mate_dev(rel))
            tell(all_ok, dev(x_peer, z * 4 + mates[rel]))
        tell(all_ok, x_dev)

    @pl.when(jnp.logical_not(herald))
    def _():
        pl.semaphore_wait(all_ok, 1)

    share(0, s1, r1)
    hand_on(1, their_z, 0)
    keep_own(1, their_z)

    finish(0, 0)
    for rel in (1, 2):
        hand_on(0, their_z, rel)
    finish(0, 1)
    for k in range(chunks):
        rows = pl.ds(k * BLOCK, BLOCK)
        pre = pre_acc[0, rows, :].astype(bf16).astype(f32)
        wide = og[rows, :].astype(f32)
        cumulative, slope = phi_and_slope(pre)
        cs[rows, :] = wide * slope
        mixed_grad = (wide * (pre * cumulative)).astype(bf16)
        mg[rows, :] = mixed_grad
        centred_grad = dot(spatial, mixed_grad, 0, 0) * gain
        cg[rows, :] = centred_grad
        turned = centred_grad.T
        s2[k:k + 1, :] = jnp.sum(turned, axis=0, keepdims=True)
        s2[chunks + k:chunks + k + 1, :] = jnp.sum(turned * gat_t[rows, :], axis=0, keepdims=True)
    share(1, s2, r2)
    hand_on(0, their_z, 0)
    keep_own(0, their_z)

    def spread(row):
        return jnp.broadcast_to(row, (BLOCK, BLOCK)).T

    def exchange(which, k):
        ref = eq.at[which, me, pl.ds(k * BLOCK, BLOCK)]
        y_sem = yg_recv.at[k] if which else c_recv.at[0]
        s_sem = sg_recv.at[k] if which else c_recv.at[1]
        send(ref, ref, e_send, y_sem, mate_dev(1))
        send(ref, ref, e_send, s_sem, mate_dev(0))

    def all_terms(which, k):
        rows = pl.ds(k * BLOCK, BLOCK)
        grads = jnp.concatenate([eq[which, q, rows, :] for q in range(4)], axis=1)
        weights = jnp.concatenate([wq[which, q].reshape(nz * BLOCK, BLOCK) for q in range(4)], axis=1)
        return dot(grads, weights, 1, 1)

    t1 = gather(0, s1, r1)
    means, invs = [], []
    mixing = jnp.zeros((BLOCK, BLOCK), f32)
    for k in range(chunks):
        rows = pl.ds(k * BLOCK, BLOCK)
        mean = t1[k:k + 1]
        inv = lax.rsqrt(t1[chunks + k:chunks + k + 1] - mean * mean + norm_eps)
        means.append(mean)
        invs.append(inv)
        inv_w = spread(inv)
        centred = (gat[rows, :] - spread(mean)) * inv_w
        centred_ref[rows, :] = centred
        slope_g[rows, :] = slope_g[rows, :] * inv_w
        normed = (centred * gain).astype(bf16)
        mixed = dot(spatial, normed, 1, 0) + bias
        eq[0, me, rows, :] = (cs[rows, :] * mixed).astype(bf16)
        exchange(0, k)
        mixing = mixing + dot(mg[rows, :], normed, 1, 1)
    mixing = jnp.where(keep, mixing, 0.0)

    def weight_part(which, t):
        at = pl.multiple_of(theirs + t * tile, tile)
        rows = pl.ds(t * tile, tile)
        gs[which, rows, :] = dot(hid_t[pl.ds(at, tile), :], eq[which, me], 1, 0).astype(bf16)
        send(gs.at[which, rows], gr.at[which, rows], gx_send.at[which], gx_recv.at[which], x_dev)

    outs = (c_out, g_out)

    def weight_own(which, t):
        at = pl.multiple_of(mine + t * tile, tile)
        outs[which][pl.ds(t * tile, tile), :] = dot(hid_t[pl.ds(at, tile), :], eq[which, me], 1, 0)

    last = pl.ds(shard, BLOCK)
    gs[0, last, :] = mixing.astype(bf16)
    send(gs.at[0, last], gr.at[0, last], gx_send.at[0], gx_recv.at[0], x_dev)
    for t in range(chunks):
        weight_part(0, t)
    for t in range(chunks):
        weight_own(0, t)

    t2 = gather(1, s2, r2)
    for k in range(chunks):
        rows = pl.ds(k * BLOCK, BLOCK)
        first = t2[k:k + 1]
        second = invs[k] * (t2[chunks + k:chunks + k + 1] - means[k] * first)
        back = cg[rows, :] - spread(first) - centred_ref[rows, :] * spread(second)
        eq[1, me, rows, :] = (back * slope_g[rows, :]).astype(bf16)
        exchange(1, k)
    for t in range(chunks):
        weight_part(1, t)
    await_bytes(eq.at[0, 0], c_recv.at[0])
    handed = eq.at[0, y_mate]
    send(handed, handed, e_send, c_recv.at[1], mate_dev(0))
    for t in range(chunks):
        weight_own(1, t)

    def z_go(slot, k, land, rsem, q):
        send(z_send.at[slot, k], r_z.at[land, k], zz_send, rsem, z_dev(q))

    def pass_on(k):
        rows = pl.ds(k * BLOCK, BLOCK)
        await_bytes(eq.at[1, 0, rows], yg_recv.at[k])
        ref = eq.at[1, y_mate, rows]
        send(ref, ref, e_send, sg_recv.at[k], mate_dev(0))

    def spread_out(k):
        await_bytes(eq.at[1, pl.ds(0, 2), pl.ds(k * BLOCK, BLOCK)], sg_recv.at[k])
        res = all_terms(1, k)
        for q in range(nz):
            part[k, q] = part[k, q] + res[:, q * BLOCK:(q + 1) * BLOCK]

        @pl.when(mid == 0)
        def _():
            for slot in range(2):
                z_send[slot, k] = part[k, z_xor[3 - slot]].astype(bf16)
                z_go(slot, k, 2 + slot, relay_recv.at[slot, k], 1)

        @pl.when(mid == 1)
        def _():
            near_end(k)

    def near_end(k):
        z_send[2, k] = part[k, z_xor[1]].astype(bf16)
        z_go(2, k, 1, zz_recv, 1)

    def relay(k):
        for slot in range(2):
            await_bytes(r_z.at[2 + slot, k], relay_recv.at[slot, k])
            z_send[1 - slot, k] = (part[k, z_xor[2 + slot]] + r_z[2 + slot, k].astype(f32)).astype(bf16)
            z_go(1 - slot, k, 0, zz_recv, 2 + slot)

    @pl.when(c == 1)
    def _():
        pass_on(0)

    await_bytes(wq.at[:, pl.ds(0, 3)], q_recv)
    await_bytes(eq.at[0, pl.ds(0, 2)], c_recv.at[1])
    for k in range(chunks):
        res = all_terms(0, k)
        for q in range(nz):
            part[k, q] = res[:, q * BLOCK:(q + 1) * BLOCK]

    @pl.when(c == 1)
    def _():
        for k in range(1, chunks):
            pass_on(k)

    for k in range(chunks):

        @pl.when(c == 0)
        def _():
            pass_on(k)

        spread_out(k)
    @pl.when(mid == 1)
    def _():
        for k in range(chunks):
            relay(k)

    @pl.when(mid == 0)
    def _():
        for k in range(chunks):
            near_end(k)

    for which in range(2):
        rows = pl.ds(0, shard + (1 - which) * BLOCK)
        await_bytes(gr.at[which, rows], gx_recv.at[which])
        for t in range(chunks):
            rows = pl.ds(t * tile, tile)
            outs[which][rows, :] = (outs[which][rows, :] + gr[which, rows, :].astype(f32)) * grad_scale
        if which == 0:
            m_out[0] = (mixing + gr[0, last, :].astype(f32)) * grad_scale

    await_bytes(r_z.at[pl.ds(0, 2)], zz_recv)
    for k in range(chunks):
        x_out[pl.ds(k * BLOCK, BLOCK), :] = (
            part[k, z] + r_z[0, k].astype(f32) + r_z[1, k].astype(f32)
        ).astype(bf16)
    await_bytes(wts.at[:, my_z], w_send)
    await_bytes(wq.at[:, pl.ds(0, 3)], q_send)
    await_bytes(r1, a_send.at[0])
    await_bytes(r2, a_send.at[1])
    await_bytes(eq.at[:, pl.ds(0, 3)], e_send)
    await_bytes(gs.at[0], gx_send.at[0])
    await_bytes(gs.at[1, pl.ds(0, shard)], gx_send.at[1])
    await_bytes(z_send, zz_send)


def store_kernel(*refs):
    count = len(refs) // 2
    src, dst, sem = refs[:count], refs[count:2 * count], refs[-1]
    stores = [pltpu.make_async_copy(src[k], dst[k], sem.at[k]) for k in range(count)]
    for store in stores:
        store.start()
    for store in stores:
        store.wait()


def fused(n_dp, hidden_in, content_weight, gating_weight, norm_gain, mixing_weight, mixing_bias, out_grad):
    toks, depth = hidden_in.shape
    shard, width = content_weight.shape
    nz = n_dp // 4
    zs = nz // 2
    chunks = toks // BLOCK
    grad_scale = 1.0 / math.sqrt(2 * toks)
    bf16, f32 = jnp.bfloat16, jnp.float32
    in_hbm = pl.BlockSpec(memory_space=pltpu.HBM)
    dma = pltpu.SemaphoreType.DMA
    once = pltpu.SemaphoreType.REGULAR
    V = pltpu.VMEM
    wide = V((toks, width), f32)
    sums = V((2 * chunks, BLOCK), f32)
    sums_in = V((n_dp - 1, 2 * chunks, BLOCK), f32)
    scratch = [
        V((1, width), f32), V((1, BLOCK, BLOCK), bf16), V((1, BLOCK), f32),
        V((toks, depth), bf16), V((depth, toks), bf16), V((2, nz, 4 * BLOCK, width), bf16),
        V((2, 4, nz, BLOCK, width), bf16), V((toks, width), bf16), V((2, toks, width), f32),
        wide, wide, wide, wide, V((toks, width), bf16), wide, wide,
        V((2, 4, toks, width), bf16), V((chunks, nz, BLOCK, width), f32),
        sums, sums_in, sums, sums_in,
        V((nz - 1, chunks, BLOCK, width), bf16), V((nz, chunks, BLOCK, width), bf16),
        V((2, shard + BLOCK, width), bf16), V((2, shard + BLOCK, width), bf16),
        dma((7,)), once, once, once, dma, dma((2, 2)), dma, dma, dma((2,)), dma((2,)),
        dma, dma((2,)), dma((chunks,)), dma((chunks,)), dma((2,)), dma((2,)), dma, dma, dma((2, chunks)),
    ]
    in_vmem = pl.BlockSpec(memory_space=V)
    results = pl.pallas_call(
        functools.partial(fused_kernel, n_dp, width * n_dp, grad_scale),
        out_shape=(
            V((toks, width), bf16),
            V((shard, width), f32),
            V((shard, width), f32),
            V(mixing_weight.shape, f32),
        ),
        in_specs=[in_hbm] * 7,
        out_specs=(in_vmem,) * 4,
        scratch_shapes=scratch,
        compiler_params=pltpu.CompilerParams(
            collective_id=0, has_side_effects=True, vmem_limit_bytes=60 * 1024 * 1024
        ),
    )(
        hidden_in, content_weight.reshape(zs, 4 * BLOCK, width), gating_weight.reshape(zs, 4 * BLOCK, width),
        norm_gain[None, :], mixing_weight, mixing_bias, out_grad,
    )
    return pl.pallas_call(
        store_kernel,
        out_shape=tuple(jax.ShapeDtypeStruct(r.shape, r.dtype) for r in results),
        in_specs=[in_vmem] * 4,
        out_specs=(in_hbm,) * 4,
        scratch_shapes=[dma((4,))],
        compiler_params=pltpu.CompilerParams(vmem_limit_bytes=60 * 1024 * 1024),
    )(*[pltpu.with_memory_space_constraint(r, V) for r in results])


def fits(n_sp, n_dp, toks, shard, width):
    paired = n_sp == 2 and n_dp == 16
    return paired and width == GROUP_DIM and shard == 2 * 4 * BLOCK and toks == 4 * BLOCK


def solve(*args):
    n_sp, n_dp = lax.axis_size("sp"), lax.axis_size("dp")
    shard, width = args[1].shape
    if fits(n_sp, n_dp, args[0].shape[0], shard, width) and args[0].shape[1] == n_dp * width:
        return fused(n_dp, *args)
    return local(*args)


def solution(mesh):
    in_specs = (
        P("sp", None),
        P("sp", "dp"),
        P("sp", "dp"),
        P("dp"),
        P("dp", None, None),
        P("dp", None),
        P("sp", "dp"),
    )
    out_specs = (P("sp", "dp"), P("sp", "dp"), P("sp", "dp"), P("dp", None, None))
    return jax.shard_map(solve, mesh=mesh, in_specs=in_specs, out_specs=out_specs, check_vma=False)
```

```python
import functools
import math

import jax
import jax.numpy as jnp
from jax import lax
from jax.experimental import pallas as pl
from jax.experimental.pallas import tpu as pltpu
from jax.sharding import PartitionSpec as P

GROUP_DIM = 128
BLOCK = 128


norm_eps = 1e-05


def gelu_slope(values):
    cumulative = 0.5 * (1.0 + lax.erf(values * (1.0 / math.sqrt(2.0))))
    density = jnp.exp(-0.5 * values * values) * (1.0 / math.sqrt(2.0 * math.pi))
    return cumulative + values * density


def causal_table(weights):
    row_ids = lax.broadcasted_iota(jnp.int32, (BLOCK, BLOCK), 0)
    col_ids = lax.broadcasted_iota(jnp.int32, (BLOCK, BLOCK), 1)
    keeper = (col_ids <= row_ids)[None]
    return (jnp.where(keeper, weights, jnp.zeros_like(weights)), keeper)


def hidden_term(hidden_in, grads):
    return lax.dot_general(
        hidden_in, grads, (((0,), (0,)), ((), ())), preferred_element_type=jnp.float32
    )


def local(
    hidden_in, content_weight, gating_weight, norm_gain, mixing_weight, mixing_bias, out_grad
):
    tok_rows = hidden_in.shape[0]
    local_width = content_weight.shape[1]
    groups_here = local_width // GROUP_DIM
    blocks = tok_rows // BLOCK
    full_width = local_width * lax.axis_size("dp")
    grad_scale = 1.0 / math.sqrt(tok_rows * lax.axis_size("sp"))
    whole_content, whole_gating = (
        lax.all_gather(content_weight, "sp", axis=0, tiled=True),
        lax.all_gather(gating_weight, "sp", axis=0, tiled=True),
    )
    joined_weight = jnp.concatenate([whole_content, whole_gating], axis=1)
    pre_both = jnp.dot(hidden_in, joined_weight, preferred_element_type=jnp.float32).astype(
        jnp.bfloat16
    )
    pre_content = pre_both[:, :local_width].astype(jnp.float32)
    pre_gating = pre_both[:, local_width:].astype(jnp.float32)
    content = jax.nn.gelu(pre_content, approximate=False)
    gating = jax.nn.gelu(pre_gating, approximate=False)
    spatial, keeper = causal_table(mixing_weight)
    grad_wide = out_grad.astype(jnp.float32)
    mixed_grad = (grad_wide * content).astype(jnp.bfloat16)
    mixed_blocks = mixed_grad.reshape(blocks, BLOCK, groups_here, GROUP_DIM)
    normed_grad = jnp.einsum(
        "gts,btgc->bsgc", spatial, mixed_blocks, preferred_element_type=jnp.float32
    )
    centred_grad = normed_grad.reshape(tok_rows, local_width) * norm_gain[None, :]
    row_sum, row_square, grad_sum, grad_raw = lax.psum(
        (
            jnp.sum(gating, axis=1),
            jnp.sum(gating * gating, axis=1),
            jnp.sum(centred_grad, axis=1),
            jnp.sum(centred_grad * gating, axis=1),
        ),
        "dp",
    )
    row_mean = (row_sum / full_width)[:, None]
    row_var = (row_square / full_width)[:, None] - row_mean * row_mean
    inv_std = lax.rsqrt(row_var + norm_eps)
    centred = (gating - row_mean) * inv_std
    first_moment = (grad_sum / full_width)[:, None]
    second_moment = inv_std * ((grad_raw / full_width)[:, None] - row_mean * first_moment)
    normed = (centred * norm_gain[None, :]).astype(jnp.bfloat16)
    normed_blocks = normed.reshape(blocks, BLOCK, groups_here, GROUP_DIM)
    mixed = jnp.einsum("gts,bsgc->btgc", spatial, normed_blocks, preferred_element_type=jnp.float32)
    mixed = (mixed + jnp.transpose(mixing_bias)[None, :, :, None]).reshape(tok_rows, local_width)
    content_pre_grad = (grad_wide * mixed * gelu_slope(pre_content)).astype(jnp.bfloat16)
    local_mixing = jnp.einsum(
        "btgc,bsgc->gts", mixed_blocks, normed_blocks, preferred_element_type=jnp.float32
    )
    local_mixing = jnp.where(keeper, local_mixing, 0.0)
    mixing_grad = lax.psum(local_mixing.astype(jnp.bfloat16), "sp").astype(jnp.float32) * grad_scale
    gating_back = inv_std * (centred_grad - first_moment - centred * second_moment)
    gating_pre_grad = (gating_back * gelu_slope(pre_gating)).astype(jnp.bfloat16)
    joined_grad = jnp.concatenate([content_pre_grad, gating_pre_grad], axis=1)
    partial_input = lax.dot_general(
        joined_grad, joined_weight, (((1,), (1,)), ((), ())), preferred_element_type=jnp.float32
    )
    input_grad = lax.psum_scatter(
        partial_input.astype(jnp.bfloat16), "dp", scatter_dimension=1, tiled=True
    )
    both_grads = (
        lax.psum_scatter(
            hidden_term(hidden_in, joined_grad).astype(jnp.bfloat16),
            "sp",
            scatter_dimension=0,
            tiled=True,
        ).astype(jnp.float32)
        * grad_scale
    )
    content_grad = both_grads[:, :local_width]
    gating_grad = both_grads[:, local_width:]
    return (input_grad, content_grad, gating_grad, mixing_grad)


def phi_and_slope(values):
    cumulative = 0.5 * (1.0 + lax.erf(values * (1.0 / math.sqrt(2.0))))
    density = jnp.exp(-0.5 * values * values) * (1.0 / math.sqrt(2.0 * math.pi))
    return cumulative, cumulative + values * density


def dot(a, b, ca, cb):
    return lax.dot_general(
        a, b, (((ca,), (cb,)), ((), ())), preferred_element_type=jnp.float32
    )


def fused_kernel(
    n_dp, full_width, grad_scale,
    h_in, wc_in, wg_in, gain_in, mix_in, bias_in, og_in,
    x_out, c_out, g_out, m_out,
    gain_ref, mix_ref, bias_ref, hid, hid_t, wts, wq, og, pre_acc,
    cs, gat, gat_t, slope_g, mg, cg, centred_ref, eq, part,
    s1, r1, s2, r2, z_send, r_z, gs, gr,
    load_sem, hello, quad_ok, all_ok, w_send, w_recv, q_send, q_recv, a_send, a_recv,
    e_send, c_recv, yg_recv, sg_recv, gx_send, gx_recv, zz_send, zz_recv, relay_recv,
):
    toks = hid.shape[0]
    chunks = toks // BLOCK
    nz = n_dp // 4
    zs = nz // 2
    shard = zs * 4 * BLOCK
    tile = shard // chunks
    bf16 = jnp.bfloat16
    f32 = jnp.float32

    i = lax.axis_index("sp")
    j = lax.axis_index("dp")
    x_peer = 1 - i
    c = lax.rem(j, 2)
    y = lax.rem(j // 2, 2)
    z = j // 4
    me = y * 2 + c
    y_mate = (1 - y) * 2 + c
    mates = (y * 2 + 1 - c, y_mate, (1 - y) * 2 + 1 - c)

    mid = lax.rem((z + 1) // 2, 2)
    z_xor = (z, z + 1 - 2 * lax.rem(z, 2), z + 2 - 4 * (z // 2), 3 - z)

    def dev(a, b):
        return {"sp": a, "dp": b}

    def mate_dev(rel):
        return dev(i, z * 4 + mates[rel])

    def z_dev(q):
        return dev(i, z_xor[q] * 4 + me)

    def remote(src, dst, ssem, rsem, target):
        return pltpu.make_async_remote_copy(
            src_ref=src, dst_ref=dst, send_sem=ssem, recv_sem=rsem,
            device_id=target, device_id_type=pl.DeviceIdType.MESH,
        )

    def send(*args):
        remote(*args).start()

    def await_bytes(ref, sem):
        pltpu.make_async_copy(ref, ref, sem).wait()

    def tell(sem, target):
        pl.semaphore_signal(sem, inc=1, device_id=target, device_id_type=pl.DeviceIdType.MESH)

    x_dev = dev(x_peer, j)
    my_z = pl.ds(zs * i, zs)
    their_z = pl.ds(zs * x_peer, zs)
    mine = pl.multiple_of(i * shard, shard)
    theirs = pl.multiple_of(x_peer * shard, shard)
    loads = [
        pltpu.make_async_copy(wg_in, wts.at[1, my_z], load_sem.at[0]),
        pltpu.make_async_copy(wc_in, wts.at[0, my_z], load_sem.at[1]),
        pltpu.make_async_copy(h_in, hid, load_sem.at[2]),
        pltpu.make_async_copy(og_in, og, load_sem.at[3]),
        pltpu.make_async_copy(gain_in, gain_ref, load_sem.at[4]),
        pltpu.make_async_copy(mix_in, mix_ref, load_sem.at[5]),
        pltpu.make_async_copy(bias_in, bias_ref, load_sem.at[6]),
    ]
    for load in loads:
        load.start()

    barrier = pltpu.get_barrier_semaphore()
    lead = i == 0
    follow = i == 1
    herald = jnp.logical_and(lead, me == 1)
    plain = jnp.logical_and(lead, me != 1)

    @pl.when(lead)
    def _():
        tell(barrier, x_dev)

    @pl.when(follow)
    def _():
        pl.semaphore_wait(barrier, 1)
        tell(hello, x_dev)

    @pl.when(lead)
    def _():
        pl.semaphore_wait(hello, 1)

    half_at = (pl.multiple_of((1 - y) * 2 * BLOCK, 2 * BLOCK), pl.multiple_of(y * 2 * BLOCK, 2 * BLOCK))

    def w_copy(which, own):
        ref = wts.at[which, my_z, pl.ds(half_at[own], 2 * BLOCK)]
        return remote(ref, ref, w_send, w_recv.at[which, own], x_dev)

    for which in (1, 0):
        loads[1 - which].wait()
        w_copy(which, 0).start()
        if which == 1:
            w_copy(1, 1).start()

    @pl.when(c == 0)
    def _():
        w_copy(0, 1).start()

    for rel in range(3):

        @pl.when(jnp.logical_and(lead, mates[rel] != 1))
        def _():
            tell(barrier, mate_dev(rel))

    @pl.when(plain)
    def _():
        pl.semaphore_wait(barrier, 3)
        tell(quad_ok, dev(i, z * 4 + 1))
        tell(hello, x_dev)

    @pl.when(herald)
    def _():
        pl.semaphore_wait(quad_ok, 3)
        tell(hello, x_dev)
        for q in range(1, nz):
            tell(barrier, z_dev(q))

    @pl.when(follow)
    def _():
        pl.semaphore_wait(hello, 1)

    others = [dev(i, lax.rem(j + k, n_dp)) for k in range(1, n_dp)]

    def hand_on(which, part_z, rel):
        at = pl.multiple_of(mates[rel] * BLOCK, BLOCK)
        send(wts.at[which, part_z, pl.ds(at, BLOCK)], wq.at[which, me, part_z], q_send, q_recv, mate_dev(rel))

    def keep_own(which, part_z):
        at = pl.multiple_of(me * BLOCK, BLOCK)
        wq[which, me, part_z] = wts[which, part_z, pl.ds(at, BLOCK)]

    for which in (1, 0):
        for rel in (1, 2, 0):
            hand_on(which, my_z, rel)

    keep = lax.broadcasted_iota(jnp.int32, (BLOCK, BLOCK), 1) <= lax.broadcasted_iota(
        jnp.int32, (BLOCK, BLOCK), 0
    )
    for load in loads[2:]:
        load.wait()
    spatial = jnp.where(keep, mix_ref[0].astype(f32), 0.0).astype(bf16)
    gain = gain_ref[...]
    bias = jnp.broadcast_to(bias_ref[...], (BLOCK, BLOCK)).T
    both = jnp.concatenate([wts[which, my_z].reshape(shard, BLOCK) for which in range(2)], axis=1)
    own = dot(hid[:, pl.ds(mine, shard)], both, 1, 0)
    pre_acc[0] = own[:, 0:BLOCK]
    pre_acc[1] = own[:, BLOCK:2 * BLOCK]
    for b in range(hid.shape[1] // BLOCK):
        hid_t[pl.ds(b * BLOCK, BLOCK), :] = hid[:, pl.ds(b * BLOCK, BLOCK)].T
    for which in range(2):
        keep_own(which, my_z)

    def finish(which, own):
        w_copy(which, own).wait_recv()
        part_sum = pre_acc[which]
        for zz in range(zs):
            at = pl.multiple_of(theirs + zz * 4 * BLOCK + half_at[own], 2 * BLOCK)
            part_sum = part_sum + dot(
                hid[:, pl.ds(at, 2 * BLOCK)],
                wts[which, zs * x_peer + zz, pl.ds(half_at[own], 2 * BLOCK)], 1, 0,
            )
        pre_acc[which] = part_sum

    def share(n, src, dst):
        for k, target in enumerate(others):
            send(src, dst.at[k], a_send.at[n], a_recv.at[n], target)

    def gather(n, src, dst):
        await_bytes(dst, a_recv.at[n])
        total = src[...]
        for k in range(len(others)):
            total = total + dst[k]
        return total * (1.0 / full_width)

    finish(1, 0)
    for rel in (1, 2):
        hand_on(1, their_z, rel)
    finish(1, 1)

    @pl.when(c == 1)
    def _():
        w_copy(0, 1).start()

    for k in range(chunks):
        rows = pl.ds(k * BLOCK, BLOCK)
        pre = pre_acc[1, rows, :].astype(bf16).astype(f32)
        cumulative, slope = phi_and_slope(pre)
        gating = pre * cumulative
        gat[rows, :] = gating
        slope_g[rows, :] = slope
        turned = gating.T
        gat_t[rows, :] = turned
        s1[k:k + 1, :] = jnp.sum(turned, axis=0, keepdims=True)
        s1[chunks + k:chunks + k + 1, :] = jnp.sum(turned * turned, axis=0, keepdims=True)

    @pl.when(herald)
    def _():
        pl.semaphore_wait(barrier, nz - 1)
        for rel in range(3):
            tell(all_ok, mate_dev(rel))
            tell(all_ok, dev(x_peer, z * 4 + mates[rel]))
        tell(all_ok, x_dev)

    @pl.when(jnp.logical_not(herald))
    def _():
        pl.semaphore_wait(all_ok, 1)

    share(0, s1, r1)
    hand_on(1, their_z, 0)
    keep_own(1, their_z)

    finish(0, 0)
    for rel in (1, 2):
        hand_on(0, their_z, rel)
    finish(0, 1)
    for k in range(chunks):
        rows = pl.ds(k * BLOCK, BLOCK)
        pre = pre_acc[0, rows, :].astype(bf16).astype(f32)
        wide = og[rows, :].astype(f32)
        cumulative, slope = phi_and_slope(pre)
        cs[rows, :] = wide * slope
        mixed_grad = (wide * (pre * cumulative)).astype(bf16)
        mg[rows, :] = mixed_grad
        centred_grad = dot(spatial, mixed_grad, 0, 0) * gain
        cg[rows, :] = centred_grad
        turned = centred_grad.T
        s2[k:k + 1, :] = jnp.sum(turned, axis=0, keepdims=True)
        s2[chunks + k:chunks + k + 1, :] = jnp.sum(turned * gat_t[rows, :], axis=0, keepdims=True)
    share(1, s2, r2)
    hand_on(0, their_z, 0)
    keep_own(0, their_z)

    def spread(row):
        return jnp.broadcast_to(row, (BLOCK, BLOCK)).T

    def exchange(which, k):
        ref = eq.at[which, me, pl.ds(k * BLOCK, BLOCK)]
        y_sem = yg_recv.at[k] if which else c_recv.at[0]
        s_sem = sg_recv.at[k] if which else c_recv.at[1]
        send(ref, ref, e_send, y_sem, mate_dev(1))
        send(ref, ref, e_send, s_sem, mate_dev(0))

    def all_terms(which, k):
        rows = pl.ds(k * BLOCK, BLOCK)
        grads = jnp.concatenate([eq[which, q, rows, :] for q in range(4)], axis=1)
        weights = jnp.concatenate([wq[which, q].reshape(nz * BLOCK, BLOCK) for q in range(4)], axis=1)
        return dot(grads, weights, 1, 1)

    t1 = gather(0, s1, r1)
    means, invs = [], []
    mixing = jnp.zeros((BLOCK, BLOCK), f32)
    for k in range(chunks):
        rows = pl.ds(k * BLOCK, BLOCK)
        mean = t1[k:k + 1]
        inv = lax.rsqrt(t1[chunks + k:chunks + k + 1] - mean * mean + norm_eps)
        means.append(mean)
        invs.append(inv)
        inv_w = spread(inv)
        centred = (gat[rows, :] - spread(mean)) * inv_w
        centred_ref[rows, :] = centred
        slope_g[rows, :] = slope_g[rows, :] * inv_w
        normed = (centred * gain).astype(bf16)
        mixed = dot(spatial, normed, 1, 0) + bias
        eq[0, me, rows, :] = (cs[rows, :] * mixed).astype(bf16)
        exchange(0, k)
        mixing = mixing + dot(mg[rows, :], normed, 1, 1)
    mixing = jnp.where(keep, mixing, 0.0)

    def weight_part(which, t):
        at = pl.multiple_of(theirs + t * tile, tile)
        rows = pl.ds(t * tile, tile)
        gs[which, rows, :] = dot(hid_t[pl.ds(at, tile), :], eq[which, me], 1, 0).astype(bf16)
        send(gs.at[which, rows], gr.at[which, rows], gx_send.at[which], gx_recv.at[which], x_dev)

    outs = (c_out, g_out)

    def weight_own(which, t):
        at = pl.multiple_of(mine + t * tile, tile)
        outs[which][pl.ds(t * tile, tile), :] = dot(hid_t[pl.ds(at, tile), :], eq[which, me], 1, 0)

    last = pl.ds(shard, BLOCK)
    gs[0, last, :] = mixing.astype(bf16)
    send(gs.at[0, last], gr.at[0, last], gx_send.at[0], gx_recv.at[0], x_dev)
    for t in range(chunks):
        weight_part(0, t)
    t2 = gather(1, s2, r2)
    for k in range(chunks):
        rows = pl.ds(k * BLOCK, BLOCK)
        first = t2[k:k + 1]
        second = invs[k] * (t2[chunks + k:chunks + k + 1] - means[k] * first)
        back = cg[rows, :] - spread(first) - centred_ref[rows, :] * spread(second)
        eq[1, me, rows, :] = (back * slope_g[rows, :]).astype(bf16)
        exchange(1, k)
    for t in range(chunks):
        weight_part(1, t)
    await_bytes(eq.at[0, 0], c_recv.at[0])
    handed = eq.at[0, y_mate]
    send(handed, handed, e_send, c_recv.at[1], mate_dev(0))
    for t in range(chunks):
        weight_own(1, t)
        weight_own(0, t)

    def z_go(slot, k, land, rsem, q):
        send(z_send.at[slot, k], r_z.at[land, k], zz_send, rsem, z_dev(q))

    def pass_on(k):
        rows = pl.ds(k * BLOCK, BLOCK)
        await_bytes(eq.at[1, 0, rows], yg_recv.at[k])
        ref = eq.at[1, y_mate, rows]
        send(ref, ref, e_send, sg_recv.at[k], mate_dev(0))

    def spread_out(k):
        await_bytes(eq.at[1, pl.ds(0, 2), pl.ds(k * BLOCK, BLOCK)], sg_recv.at[k])
        res = all_terms(1, k)
        for q in range(nz):
            part[k, q] = part[k, q] + res[:, q * BLOCK:(q + 1) * BLOCK]

        @pl.when(mid == 0)
        def _():
            for slot in range(2):
                z_send[slot, k] = part[k, z_xor[3 - slot]].astype(bf16)
                z_go(slot, k, 2 + slot, relay_recv.at[slot, k], 1)

        @pl.when(mid == 1)
        def _():
            near_end(k)

    def near_end(k):
        z_send[2, k] = part[k, z_xor[1]].astype(bf16)
        z_go(2, k, 1, zz_recv, 1)

    def relay(k):
        for slot in range(2):
            await_bytes(r_z.at[2 + slot, k], relay_recv.at[slot, k])
            z_send[1 - slot, k] = (part[k, z_xor[2 + slot]] + r_z[2 + slot, k].astype(f32)).astype(bf16)
            z_go(1 - slot, k, 0, zz_recv, 2 + slot)

    @pl.when(c == 1)
    def _():
        pass_on(0)

    await_bytes(wq.at[:, pl.ds(0, 3)], q_recv)
    await_bytes(eq.at[0, pl.ds(0, 2)], c_recv.at[1])
    for k in range(chunks):
        res = all_terms(0, k)
        for q in range(nz):
            part[k, q] = res[:, q * BLOCK:(q + 1) * BLOCK]

    @pl.when(c == 1)
    def _():
        for k in range(1, chunks):
            pass_on(k)

    for k in range(chunks):

        @pl.when(c == 0)
        def _():
            pass_on(k)

        spread_out(k)
    @pl.when(mid == 1)
    def _():
        for k in range(chunks):
            relay(k)

    @pl.when(mid == 0)
    def _():
        for k in range(chunks):
            near_end(k)

    for which in range(2):
        rows = pl.ds(0, shard + (1 - which) * BLOCK)
        await_bytes(gr.at[which, rows], gx_recv.at[which])
        for t in range(chunks):
            rows = pl.ds(t * tile, tile)
            outs[which][rows, :] = (outs[which][rows, :] + gr[which, rows, :].astype(f32)) * grad_scale
        if which == 0:
            m_out[0] = (mixing + gr[0, last, :].astype(f32)) * grad_scale

    await_bytes(r_z.at[pl.ds(0, 2)], zz_recv)
    for k in range(chunks):
        x_out[pl.ds(k * BLOCK, BLOCK), :] = (
            part[k, z] + r_z[0, k].astype(f32) + r_z[1, k].astype(f32)
        ).astype(bf16)
    await_bytes(wts.at[:, my_z], w_send)
    await_bytes(wq.at[:, pl.ds(0, 3)], q_send)
    await_bytes(r1, a_send.at[0])
    await_bytes(r2, a_send.at[1])
    await_bytes(eq.at[:, pl.ds(0, 3)], e_send)
    await_bytes(gs.at[0], gx_send.at[0])
    await_bytes(gs.at[1, pl.ds(0, shard)], gx_send.at[1])
    await_bytes(z_send, zz_send)


def store_kernel(*refs):
    count = len(refs) // 2
    src, dst, sem = refs[:count], refs[count:2 * count], refs[-1]
    stores = [pltpu.make_async_copy(src[k], dst[k], sem.at[k]) for k in range(count)]
    for store in stores:
        store.start()
    for store in stores:
        store.wait()


def fused(n_dp, hidden_in, content_weight, gating_weight, norm_gain, mixing_weight, mixing_bias, out_grad):
    toks, depth = hidden_in.shape
    shard, width = content_weight.shape
    nz = n_dp // 4
    zs = nz // 2
    chunks = toks // BLOCK
    grad_scale = 1.0 / math.sqrt(2 * toks)
    bf16, f32 = jnp.bfloat16, jnp.float32
    in_hbm = pl.BlockSpec(memory_space=pltpu.HBM)
    dma = pltpu.SemaphoreType.DMA
    once = pltpu.SemaphoreType.REGULAR
    V = pltpu.VMEM
    wide = V((toks, width), f32)
    sums = V((2 * chunks, BLOCK), f32)
    sums_in = V((n_dp - 1, 2 * chunks, BLOCK), f32)
    scratch = [
        V((1, width), f32), V((1, BLOCK, BLOCK), bf16), V((1, BLOCK), f32),
        V((toks, depth), bf16), V((depth, toks), bf16), V((2, nz, 4 * BLOCK, width), bf16),
        V((2, 4, nz, BLOCK, width), bf16), V((toks, width), bf16), V((2, toks, width), f32),
        wide, wide, wide, wide, V((toks, width), bf16), wide, wide,
        V((2, 4, toks, width), bf16), V((chunks, nz, BLOCK, width), f32),
        sums, sums_in, sums, sums_in,
        V((nz - 1, chunks, BLOCK, width), bf16), V((nz, chunks, BLOCK, width), bf16),
        V((2, shard + BLOCK, width), bf16), V((2, shard + BLOCK, width), bf16),
        dma((7,)), once, once, once, dma, dma((2, 2)), dma, dma, dma((2,)), dma((2,)),
        dma, dma((2,)), dma((chunks,)), dma((chunks,)), dma((2,)), dma((2,)), dma, dma, dma((2, chunks)),
    ]
    in_vmem = pl.BlockSpec(memory_space=V)
    results = pl.pallas_call(
        functools.partial(fused_kernel, n_dp, width * n_dp, grad_scale),
        out_shape=(
            V((toks, width), bf16),
            V((shard, width), f32),
            V((shard, width), f32),
            V(mixing_weight.shape, f32),
        ),
        in_specs=[in_hbm] * 7,
        out_specs=(in_vmem,) * 4,
        scratch_shapes=scratch,
        compiler_params=pltpu.CompilerParams(
            collective_id=0, has_side_effects=True, vmem_limit_bytes=60 * 1024 * 1024
        ),
    )(
        hidden_in, content_weight.reshape(zs, 4 * BLOCK, width), gating_weight.reshape(zs, 4 * BLOCK, width),
        norm_gain[None, :], mixing_weight, mixing_bias, out_grad,
    )
    return pl.pallas_call(
        store_kernel,
        out_shape=tuple(jax.ShapeDtypeStruct(r.shape, r.dtype) for r in results),
        in_specs=[in_vmem] * 4,
        out_specs=(in_hbm,) * 4,
        scratch_shapes=[dma((4,))],
        compiler_params=pltpu.CompilerParams(vmem_limit_bytes=60 * 1024 * 1024),
    )(*[pltpu.with_memory_space_constraint(r, V) for r in results])


def fits(n_sp, n_dp, toks, shard, width):
    paired = n_sp == 2 and n_dp == 16
    return paired and width == GROUP_DIM and shard == 2 * 4 * BLOCK and toks == 4 * BLOCK


def solve(*args):
    n_sp, n_dp = lax.axis_size("sp"), lax.axis_size("dp")
    shard, width = args[1].shape
    if fits(n_sp, n_dp, args[0].shape[0], shard, width) and args[0].shape[1] == n_dp * width:
        return fused(n_dp, *args)
    return local(*args)


def solution(mesh):
    in_specs = (
        P("sp", None),
        P("sp", "dp"),
        P("sp", "dp"),
        P("dp"),
        P("dp", None, None),
        P("dp", None),
        P("sp", "dp"),
    )
    out_specs = (P("sp", "dp"), P("sp", "dp"), P("sp", "dp"), P("dp", None, None))
    return jax.shard_map(solve, mesh=mesh, in_specs=in_specs, out_specs=out_specs, check_vma=False)
```

```python
import functools
import math

import jax
import jax.numpy as jnp
from jax import lax
from jax.experimental import pallas as pl
from jax.experimental.pallas import tpu as pltpu
from jax.sharding import PartitionSpec as P

GROUP_DIM = 128
BLOCK = 128


norm_eps = 1e-05


def gelu_slope(values):
    cumulative = 0.5 * (1.0 + lax.erf(values * (1.0 / math.sqrt(2.0))))
    density = jnp.exp(-0.5 * values * values) * (1.0 / math.sqrt(2.0 * math.pi))
    return cumulative + values * density


def causal_table(weights):
    row_ids = lax.broadcasted_iota(jnp.int32, (BLOCK, BLOCK), 0)
    col_ids = lax.broadcasted_iota(jnp.int32, (BLOCK, BLOCK), 1)
    keeper = (col_ids <= row_ids)[None]
    return (jnp.where(keeper, weights, jnp.zeros_like(weights)), keeper)


def hidden_term(hidden_in, grads):
    return lax.dot_general(
        hidden_in, grads, (((0,), (0,)), ((), ())), preferred_element_type=jnp.float32
    )


def local(
    hidden_in, content_weight, gating_weight, norm_gain, mixing_weight, mixing_bias, out_grad
):
    tok_rows = hidden_in.shape[0]
    local_width = content_weight.shape[1]
    groups_here = local_width // GROUP_DIM
    blocks = tok_rows // BLOCK
    full_width = local_width * lax.axis_size("dp")
    grad_scale = 1.0 / math.sqrt(tok_rows * lax.axis_size("sp"))
    whole_content, whole_gating = (
        lax.all_gather(content_weight, "sp", axis=0, tiled=True),
        lax.all_gather(gating_weight, "sp", axis=0, tiled=True),
    )
    joined_weight = jnp.concatenate([whole_content, whole_gating], axis=1)
    pre_both = jnp.dot(hidden_in, joined_weight, preferred_element_type=jnp.float32).astype(
        jnp.bfloat16
    )
    pre_content = pre_both[:, :local_width].astype(jnp.float32)
    pre_gating = pre_both[:, local_width:].astype(jnp.float32)
    content = jax.nn.gelu(pre_content, approximate=False)
    gating = jax.nn.gelu(pre_gating, approximate=False)
    spatial, keeper = causal_table(mixing_weight)
    grad_wide = out_grad.astype(jnp.float32)
    mixed_grad = (grad_wide * content).astype(jnp.bfloat16)
    mixed_blocks = mixed_grad.reshape(blocks, BLOCK, groups_here, GROUP_DIM)
    normed_grad = jnp.einsum(
        "gts,btgc->bsgc", spatial, mixed_blocks, preferred_element_type=jnp.float32
    )
    centred_grad = normed_grad.reshape(tok_rows, local_width) * norm_gain[None, :]
    row_sum, row_square, grad_sum, grad_raw = lax.psum(
        (
            jnp.sum(gating, axis=1),
            jnp.sum(gating * gating, axis=1),
            jnp.sum(centred_grad, axis=1),
            jnp.sum(centred_grad * gating, axis=1),
        ),
        "dp",
    )
    row_mean = (row_sum / full_width)[:, None]
    row_var = (row_square / full_width)[:, None] - row_mean * row_mean
    inv_std = lax.rsqrt(row_var + norm_eps)
    centred = (gating - row_mean) * inv_std
    first_moment = (grad_sum / full_width)[:, None]
    second_moment = inv_std * ((grad_raw / full_width)[:, None] - row_mean * first_moment)
    normed = (centred * norm_gain[None, :]).astype(jnp.bfloat16)
    normed_blocks = normed.reshape(blocks, BLOCK, groups_here, GROUP_DIM)
    mixed = jnp.einsum("gts,bsgc->btgc", spatial, normed_blocks, preferred_element_type=jnp.float32)
    mixed = (mixed + jnp.transpose(mixing_bias)[None, :, :, None]).reshape(tok_rows, local_width)
    content_pre_grad = (grad_wide * mixed * gelu_slope(pre_content)).astype(jnp.bfloat16)
    local_mixing = jnp.einsum(
        "btgc,bsgc->gts", mixed_blocks, normed_blocks, preferred_element_type=jnp.float32
    )
    local_mixing = jnp.where(keeper, local_mixing, 0.0)
    mixing_grad = lax.psum(local_mixing.astype(jnp.bfloat16), "sp").astype(jnp.float32) * grad_scale
    gating_back = inv_std * (centred_grad - first_moment - centred * second_moment)
    gating_pre_grad = (gating_back * gelu_slope(pre_gating)).astype(jnp.bfloat16)
    joined_grad = jnp.concatenate([content_pre_grad, gating_pre_grad], axis=1)
    partial_input = lax.dot_general(
        joined_grad, joined_weight, (((1,), (1,)), ((), ())), preferred_element_type=jnp.float32
    )
    input_grad = lax.psum_scatter(
        partial_input.astype(jnp.bfloat16), "dp", scatter_dimension=1, tiled=True
    )
    both_grads = (
        lax.psum_scatter(
            hidden_term(hidden_in, joined_grad).astype(jnp.bfloat16),
            "sp",
            scatter_dimension=0,
            tiled=True,
        ).astype(jnp.float32)
        * grad_scale
    )
    content_grad = both_grads[:, :local_width]
    gating_grad = both_grads[:, local_width:]
    return (input_grad, content_grad, gating_grad, mixing_grad)


def phi_and_slope(values):
    cumulative = 0.5 * (1.0 + lax.erf(values * (1.0 / math.sqrt(2.0))))
    density = jnp.exp(-0.5 * values * values) * (1.0 / math.sqrt(2.0 * math.pi))
    return cumulative, cumulative + values * density


def dot(a, b, ca, cb):
    return lax.dot_general(
        a, b, (((ca,), (cb,)), ((), ())), preferred_element_type=jnp.float32
    )


def fused_kernel(
    n_dp, full_width, grad_scale,
    h_in, wc_in, wg_in, gain_in, mix_in, bias_in, og_in,
    x_out, c_out, g_out, m_out,
    gain_ref, mix_ref, bias_ref, hid, hid_t, wts, wq, og, pre_acc,
    cs, gat, gat_t, slope_g, mg, cg, centred_ref, eq, part,
    s1, r1, s2, r2, z_send, r_z, gs, gr,
    load_sem, hello, quad_ok, all_ok, w_send, w_recv, q_send, q_recv, a_send, a_recv,
    e_send, c_recv, yg_recv, sg_recv, gx_send, gx_recv, zz_send, zz_recv, relay_recv,
):
    toks = hid.shape[0]
    chunks = toks // BLOCK
    nz = n_dp // 4
    zs = nz // 2
    shard = zs * 4 * BLOCK
    tile = shard // chunks
    bf16 = jnp.bfloat16
    f32 = jnp.float32

    i = lax.axis_index("sp")
    j = lax.axis_index("dp")
    x_peer = 1 - i
    c = lax.rem(j, 2)
    y = lax.rem(j // 2, 2)
    z = j // 4
    me = y * 2 + c
    y_mate = (1 - y) * 2 + c
    mates = (y * 2 + 1 - c, y_mate, (1 - y) * 2 + 1 - c)

    mid = lax.rem((z + 1) // 2, 2)
    z_xor = (z, z + 1 - 2 * lax.rem(z, 2), z + 2 - 4 * (z // 2), 3 - z)

    def dev(a, b):
        return {"sp": a, "dp": b}

    def mate_dev(rel):
        return dev(i, z * 4 + mates[rel])

    def z_dev(q):
        return dev(i, z_xor[q] * 4 + me)

    def remote(src, dst, ssem, rsem, target):
        return pltpu.make_async_remote_copy(
            src_ref=src, dst_ref=dst, send_sem=ssem, recv_sem=rsem,
            device_id=target, device_id_type=pl.DeviceIdType.MESH,
        )

    def send(*args):
        remote(*args).start()

    def await_bytes(ref, sem):
        pltpu.make_async_copy(ref, ref, sem).wait()

    def tell(sem, target):
        pl.semaphore_signal(sem, inc=1, device_id=target, device_id_type=pl.DeviceIdType.MESH)

    x_dev = dev(x_peer, j)
    my_z = pl.ds(zs * i, zs)
    their_z = pl.ds(zs * x_peer, zs)
    mine = pl.multiple_of(i * shard, shard)
    theirs = pl.multiple_of(x_peer * shard, shard)
    loads = [
        pltpu.make_async_copy(wg_in, wts.at[1, my_z], load_sem.at[0]),
        pltpu.make_async_copy(wc_in, wts.at[0, my_z], load_sem.at[1]),
        pltpu.make_async_copy(h_in, hid, load_sem.at[2]),
        pltpu.make_async_copy(og_in, og, load_sem.at[3]),
        pltpu.make_async_copy(gain_in, gain_ref, load_sem.at[4]),
        pltpu.make_async_copy(mix_in, mix_ref, load_sem.at[5]),
        pltpu.make_async_copy(bias_in, bias_ref, load_sem.at[6]),
    ]
    for load in loads:
        load.start()

    barrier = pltpu.get_barrier_semaphore()
    lead = i == 0
    follow = i == 1
    herald = jnp.logical_and(lead, me == 1)
    plain = jnp.logical_and(lead, me != 1)

    @pl.when(lead)
    def _():
        tell(barrier, x_dev)

    @pl.when(follow)
    def _():
        pl.semaphore_wait(barrier, 1)
        tell(hello, x_dev)

    @pl.when(lead)
    def _():
        pl.semaphore_wait(hello, 1)

    half_at = (pl.multiple_of((1 - y) * 2 * BLOCK, 2 * BLOCK), pl.multiple_of(y * 2 * BLOCK, 2 * BLOCK))

    def w_copy(which, own):
        ref = wts.at[which, my_z, pl.ds(half_at[own], 2 * BLOCK)]
        return remote(ref, ref, w_send, w_recv.at[which, own], x_dev)

    for which in (1, 0):
        loads[1 - which].wait()
        w_copy(which, 0).start()
        if which == 1:
            w_copy(1, 1).start()

    @pl.when(c == 0)
    def _():
        w_copy(0, 1).start()

    for rel in range(3):

        @pl.when(jnp.logical_and(lead, mates[rel] != 1))
        def _():
            tell(barrier, mate_dev(rel))

    @pl.when(plain)
    def _():
        pl.semaphore_wait(barrier, 3)
        tell(quad_ok, dev(i, z * 4 + 1))
        tell(hello, x_dev)

    @pl.when(herald)
    def _():
        pl.semaphore_wait(quad_ok, 3)
        tell(hello, x_dev)
        for q in range(1, nz):
            tell(barrier, z_dev(q))

    @pl.when(follow)
    def _():
        pl.semaphore_wait(hello, 1)

    others = [dev(i, lax.rem(j + k, n_dp)) for k in range(1, n_dp)]

    def hand_on(which, part_z, rel):
        at = pl.multiple_of(mates[rel] * BLOCK, BLOCK)
        send(wts.at[which, part_z, pl.ds(at, BLOCK)], wq.at[which, me, part_z], q_send, q_recv, mate_dev(rel))

    def keep_own(which, part_z):
        at = pl.multiple_of(me * BLOCK, BLOCK)
        wq[which, me, part_z] = wts[which, part_z, pl.ds(at, BLOCK)]

    for which in (1, 0):
        for rel in (1, 2, 0):
            hand_on(which, my_z, rel)

    keep = lax.broadcasted_iota(jnp.int32, (BLOCK, BLOCK), 1) <= lax.broadcasted_iota(
        jnp.int32, (BLOCK, BLOCK), 0
    )
    for load in loads[2:]:
        load.wait()
    spatial = jnp.where(keep, mix_ref[0].astype(f32), 0.0).astype(bf16)
    gain = gain_ref[...]
    bias = jnp.broadcast_to(bias_ref[...], (BLOCK, BLOCK)).T
    both = jnp.concatenate([wts[which, my_z].reshape(shard, BLOCK) for which in range(2)], axis=1)
    own = dot(hid[:, pl.ds(mine, shard)], both, 1, 0)
    pre_acc[0] = own[:, 0:BLOCK]
    pre_acc[1] = own[:, BLOCK:2 * BLOCK]
    for b in range(hid.shape[1] // BLOCK):
        hid_t[pl.ds(b * BLOCK, BLOCK), :] = hid[:, pl.ds(b * BLOCK, BLOCK)].T
    for which in range(2):
        keep_own(which, my_z)

    def finish(which, own):
        w_copy(which, own).wait_recv()
        part_sum = pre_acc[which]
        for zz in range(zs):
            at = pl.multiple_of(theirs + zz * 4 * BLOCK + half_at[own], 2 * BLOCK)
            part_sum = part_sum + dot(
                hid[:, pl.ds(at, 2 * BLOCK)],
                wts[which, zs * x_peer + zz, pl.ds(half_at[own], 2 * BLOCK)], 1, 0,
            )
        pre_acc[which] = part_sum

    def share(n, src, dst):
        for k, target in enumerate(others):
            send(src, dst.at[k], a_send.at[n], a_recv.at[n], target)

    def gather(n, src, dst):
        await_bytes(dst, a_recv.at[n])
        total = src[...]
        for k in range(len(others)):
            total = total + dst[k]
        return total * (1.0 / full_width)

    finish(1, 0)
    for rel in (1, 2):
        hand_on(1, their_z, rel)
    finish(1, 1)

    @pl.when(c == 1)
    def _():
        w_copy(0, 1).start()

    for k in range(chunks):
        rows = pl.ds(k * BLOCK, BLOCK)
        pre = pre_acc[1, rows, :].astype(bf16).astype(f32)
        cumulative, slope = phi_and_slope(pre)
        gating = pre * cumulative
        gat[rows, :] = gating
        slope_g[rows, :] = slope
        turned = gating.T
        gat_t[rows, :] = turned
        s1[k:k + 1, :] = jnp.sum(turned, axis=0, keepdims=True)
        s1[chunks + k:chunks + k + 1, :] = jnp.sum(turned * turned, axis=0, keepdims=True)

    @pl.when(herald)
    def _():
        pl.semaphore_wait(barrier, nz - 1)
        for rel in range(3):
            tell(all_ok, mate_dev(rel))
            tell(all_ok, dev(x_peer, z * 4 + mates[rel]))
        tell(all_ok, x_dev)

    @pl.when(jnp.logical_not(herald))
    def _():
        pl.semaphore_wait(all_ok, 1)

    share(0, s1, r1)
    hand_on(1, their_z, 0)
    keep_own(1, their_z)

    finish(0, 0)
    for rel in (1, 2):
        hand_on(0, their_z, rel)
    finish(0, 1)
    for k in range(chunks):
        rows = pl.ds(k * BLOCK, BLOCK)
        pre = pre_acc[0, rows, :].astype(bf16).astype(f32)
        wide = og[rows, :].astype(f32)
        cumulative, slope = phi_and_slope(pre)
        cs[rows, :] = wide * slope
        mixed_grad = (wide * (pre * cumulative)).astype(bf16)
        mg[rows, :] = mixed_grad
        centred_grad = dot(spatial, mixed_grad, 0, 0) * gain
        cg[rows, :] = centred_grad
        turned = centred_grad.T
        s2[k:k + 1, :] = jnp.sum(turned, axis=0, keepdims=True)
        s2[chunks + k:chunks + k + 1, :] = jnp.sum(turned * gat_t[rows, :], axis=0, keepdims=True)
    share(1, s2, r2)
    hand_on(0, their_z, 0)
    keep_own(0, their_z)

    def spread(row):
        return jnp.broadcast_to(row, (BLOCK, BLOCK)).T

    def exchange(which, k):
        ref = eq.at[which, me, pl.ds(k * BLOCK, BLOCK)]
        y_sem = yg_recv.at[k] if which else c_recv.at[0]
        s_sem = sg_recv.at[k] if which else c_recv.at[1]
        send(ref, ref, e_send, y_sem, mate_dev(1))
        send(ref, ref, e_send, s_sem, mate_dev(0))

    def all_terms(which, k):
        rows = pl.ds(k * BLOCK, BLOCK)
        grads = jnp.concatenate([eq[which, q, rows, :] for q in range(4)], axis=1)
        weights = jnp.concatenate([wq[which, q].reshape(nz * BLOCK, BLOCK) for q in range(4)], axis=1)
        return dot(grads, weights, 1, 1)

    t1 = gather(0, s1, r1)
    means, invs = [], []
    mixing = jnp.zeros((BLOCK, BLOCK), f32)
    for k in range(chunks):
        rows = pl.ds(k * BLOCK, BLOCK)
        mean = t1[k:k + 1]
        inv = lax.rsqrt(t1[chunks + k:chunks + k + 1] - mean * mean + norm_eps)
        means.append(mean)
        invs.append(inv)
        inv_w = spread(inv)
        centred = (gat[rows, :] - spread(mean)) * inv_w
        centred_ref[rows, :] = centred
        slope_g[rows, :] = slope_g[rows, :] * inv_w
        normed = (centred * gain).astype(bf16)
        mixed = dot(spatial, normed, 1, 0) + bias
        eq[0, me, rows, :] = (cs[rows, :] * mixed).astype(bf16)
        exchange(0, k)
        mixing = mixing + dot(mg[rows, :], normed, 1, 1)
    mixing = jnp.where(keep, mixing, 0.0)

    def weight_part(which, t):
        at = pl.multiple_of(theirs + t * tile, tile)
        rows = pl.ds(t * tile, tile)
        gs[which, rows, :] = dot(hid_t[pl.ds(at, tile), :], eq[which, me], 1, 0).astype(bf16)
        send(gs.at[which, rows], gr.at[which, rows], gx_send.at[which], gx_recv.at[which], x_dev)

    outs = (c_out, g_out)

    def weight_own(which, t):
        at = pl.multiple_of(mine + t * tile, tile)
        outs[which][pl.ds(t * tile, tile), :] = dot(hid_t[pl.ds(at, tile), :], eq[which, me], 1, 0)

    last = pl.ds(shard, BLOCK)
    gs[0, last, :] = mixing.astype(bf16)
    send(gs.at[0, last], gr.at[0, last], gx_send.at[0], gx_recv.at[0], x_dev)
    for t in range(chunks):
        weight_part(0, t)
    t2 = gather(1, s2, r2)
    for k in range(chunks):
        rows = pl.ds(k * BLOCK, BLOCK)
        first = t2[k:k + 1]
        second = invs[k] * (t2[chunks + k:chunks + k + 1] - means[k] * first)
        back = cg[rows, :] - spread(first) - centred_ref[rows, :] * spread(second)
        eq[1, me, rows, :] = (back * slope_g[rows, :]).astype(bf16)
        exchange(1, k)
    for t in range(chunks):
        weight_part(1, t)
    await_bytes(eq.at[0, 0], c_recv.at[0])
    handed = eq.at[0, y_mate]
    send(handed, handed, e_send, c_recv.at[1], mate_dev(0))
    for t in range(chunks):
        weight_own(1, t)
        weight_own(0, t)

    def z_go(slot, k, land, rsem, q):
        send(z_send.at[slot, k], r_z.at[land, k], zz_send, rsem, z_dev(q))

    def pass_on(k):
        rows = pl.ds(k * BLOCK, BLOCK)
        await_bytes(eq.at[1, 0, rows], yg_recv.at[k])
        ref = eq.at[1, y_mate, rows]
        send(ref, ref, e_send, sg_recv.at[k], mate_dev(0))

    def spread_out(k):
        await_bytes(eq.at[1, pl.ds(0, 2), pl.ds(k * BLOCK, BLOCK)], sg_recv.at[k])
        res = all_terms(1, k)
        for q in range(nz):
            part[k, q] = part[k, q] + res[:, q * BLOCK:(q + 1) * BLOCK]

        @pl.when(mid == 0)
        def _():
            for slot in range(2):
                z_send[slot, k] = part[k, z_xor[3 - slot]].astype(bf16)
                z_go(slot, k, 2 + slot, relay_recv.at[slot, k], 1)
            if k == 0:
                near_end(k)

        @pl.when(mid == 1)
        def _():
            near_end(k)

    def near_end(k):
        z_send[2, k] = part[k, z_xor[1]].astype(bf16)
        z_go(2, k, 1, zz_recv, 1)

    def relay(k):
        for slot in range(2):
            await_bytes(r_z.at[2 + slot, k], relay_recv.at[slot, k])
            z_send[1 - slot, k] = (part[k, z_xor[2 + slot]] + r_z[2 + slot, k].astype(f32)).astype(bf16)
            z_go(1 - slot, k, 0, zz_recv, 2 + slot)

    @pl.when(c == 1)
    def _():
        pass_on(0)

    await_bytes(wq.at[:, pl.ds(0, 3)], q_recv)
    await_bytes(eq.at[0, pl.ds(0, 2)], c_recv.at[1])
    for k in range(chunks):
        res = all_terms(0, k)
        for q in range(nz):
            part[k, q] = res[:, q * BLOCK:(q + 1) * BLOCK]

    @pl.when(c == 1)
    def _():
        for k in range(1, chunks):
            pass_on(k)

    for k in range(chunks):

        @pl.when(c == 0)
        def _():
            pass_on(k)

        spread_out(k)
    @pl.when(mid == 1)
    def _():
        for k in range(chunks):
            relay(k)

    @pl.when(mid == 0)
    def _():
        for k in range(1, chunks):
            near_end(k)

    for which in range(2):
        rows = pl.ds(0, shard + (1 - which) * BLOCK)
        await_bytes(gr.at[which, rows], gx_recv.at[which])
        for t in range(chunks):
            rows = pl.ds(t * tile, tile)
            outs[which][rows, :] = (outs[which][rows, :] + gr[which, rows, :].astype(f32)) * grad_scale
        if which == 0:
            m_out[0] = (mixing + gr[0, last, :].astype(f32)) * grad_scale

    await_bytes(r_z.at[pl.ds(0, 2)], zz_recv)
    for k in range(chunks):
        x_out[pl.ds(k * BLOCK, BLOCK), :] = (
            part[k, z] + r_z[0, k].astype(f32) + r_z[1, k].astype(f32)
        ).astype(bf16)
    await_bytes(wts.at[:, my_z], w_send)
    await_bytes(wq.at[:, pl.ds(0, 3)], q_send)
    await_bytes(r1, a_send.at[0])
    await_bytes(r2, a_send.at[1])
    await_bytes(eq.at[:, pl.ds(0, 3)], e_send)
    await_bytes(gs.at[0], gx_send.at[0])
    await_bytes(gs.at[1, pl.ds(0, shard)], gx_send.at[1])
    await_bytes(z_send, zz_send)


def store_kernel(*refs):
    count = len(refs) // 2
    src, dst, sem = refs[:count], refs[count:2 * count], refs[-1]
    stores = [pltpu.make_async_copy(src[k], dst[k], sem.at[k]) for k in range(count)]
    for store in stores:
        store.start()
    for store in stores:
        store.wait()


def fused(n_dp, hidden_in, content_weight, gating_weight, norm_gain, mixing_weight, mixing_bias, out_grad):
    toks, depth = hidden_in.shape
    shard, width = content_weight.shape
    nz = n_dp // 4
    zs = nz // 2
    chunks = toks // BLOCK
    grad_scale = 1.0 / math.sqrt(2 * toks)
    bf16, f32 = jnp.bfloat16, jnp.float32
    in_hbm = pl.BlockSpec(memory_space=pltpu.HBM)
    dma = pltpu.SemaphoreType.DMA
    once = pltpu.SemaphoreType.REGULAR
    V = pltpu.VMEM
    wide = V((toks, width), f32)
    sums = V((2 * chunks, BLOCK), f32)
    sums_in = V((n_dp - 1, 2 * chunks, BLOCK), f32)
    scratch = [
        V((1, width), f32), V((1, BLOCK, BLOCK), bf16), V((1, BLOCK), f32),
        V((toks, depth), bf16), V((depth, toks), bf16), V((2, nz, 4 * BLOCK, width), bf16),
        V((2, 4, nz, BLOCK, width), bf16), V((toks, width), bf16), V((2, toks, width), f32),
        wide, wide, wide, wide, V((toks, width), bf16), wide, wide,
        V((2, 4, toks, width), bf16), V((chunks, nz, BLOCK, width), f32),
        sums, sums_in, sums, sums_in,
        V((nz - 1, chunks, BLOCK, width), bf16), V((nz, chunks, BLOCK, width), bf16),
        V((2, shard + BLOCK, width), bf16), V((2, shard + BLOCK, width), bf16),
        dma((7,)), once, once, once, dma, dma((2, 2)), dma, dma, dma((2,)), dma((2,)),
        dma, dma((2,)), dma((chunks,)), dma((chunks,)), dma((2,)), dma((2,)), dma, dma, dma((2, chunks)),
    ]
    in_vmem = pl.BlockSpec(memory_space=V)
    results = pl.pallas_call(
        functools.partial(fused_kernel, n_dp, width * n_dp, grad_scale),
        out_shape=(
            V((toks, width), bf16),
            V((shard, width), f32),
            V((shard, width), f32),
            V(mixing_weight.shape, f32),
        ),
        in_specs=[in_hbm] * 7,
        out_specs=(in_vmem,) * 4,
        scratch_shapes=scratch,
        compiler_params=pltpu.CompilerParams(
            collective_id=0, has_side_effects=True, vmem_limit_bytes=60 * 1024 * 1024
        ),
    )(
        hidden_in, content_weight.reshape(zs, 4 * BLOCK, width), gating_weight.reshape(zs, 4 * BLOCK, width),
        norm_gain[None, :], mixing_weight, mixing_bias, out_grad,
    )
    return pl.pallas_call(
        store_kernel,
        out_shape=tuple(jax.ShapeDtypeStruct(r.shape, r.dtype) for r in results),
        in_specs=[in_vmem] * 4,
        out_specs=(in_hbm,) * 4,
        scratch_shapes=[dma((4,))],
        compiler_params=pltpu.CompilerParams(vmem_limit_bytes=60 * 1024 * 1024),
    )(*[pltpu.with_memory_space_constraint(r, V) for r in results])


def fits(n_sp, n_dp, toks, shard, width):
    paired = n_sp == 2 and n_dp == 16
    return paired and width == GROUP_DIM and shard == 2 * 4 * BLOCK and toks == 4 * BLOCK


def solve(*args):
    n_sp, n_dp = lax.axis_size("sp"), lax.axis_size("dp")
    shard, width = args[1].shape
    if fits(n_sp, n_dp, args[0].shape[0], shard, width) and args[0].shape[1] == n_dp * width:
        return fused(n_dp, *args)
    return local(*args)


def solution(mesh):
    in_specs = (
        P("sp", None),
        P("sp", "dp"),
        P("sp", "dp"),
        P("dp"),
        P("dp", None, None),
        P("dp", None),
        P("sp", "dp"),
    )
    out_specs = (P("sp", "dp"), P("sp", "dp"), P("sp", "dp"), P("dp", None, None))
    return jax.shard_map(solve, mesh=mesh, in_specs=in_specs, out_specs=out_specs, check_vma=False)
```
